512 devices in a mesh: ep: 32 (over z, core), tp: 16 (over y, x).
Axes of the slice: x: 4, y: 4, z: 16, core: 2. Of those that a mesh axis runs over, the one named last changes fastest.
Arguments:
- tokens: bfloat16 [8192, 2048], P('ep', 'tp'), may hold values from -800 to 800
- norm_gain: bfloat16 [2048], P('tp'), may hold values from 0.099609375 to 1.8984375
- w_gate: bfloat16 [32, 2048, 6144], P('ep', None, 'tp'), may hold values from -0.125 to 0.125
- w_up: bfloat16 [32, 2048, 6144], P('ep', None, 'tp'), may hold values from -0.125 to 0.125
- w_down: bfloat16 [32, 6144, 2048], P('ep', 'tp'), may hold values from -1.2757759 to 1.2757759
- routes: int32 [8192, 2], P('ep'), may hold values from 0 to 31, all different within a row; in each aligned block of 256 rows (0 to 255, 256 to 511, ...) at most 32 rows name the same one
- route_weights: float32 [8192, 2], P('ep'), may hold values from 0.1 to 1
- final_gain: bfloat16 [2048], P('tp'), may hold values from 0.099609375 to 1.8984375
Outputs:
- mixed_out: bfloat16 [8192, 2048], P('ep', 'tp')
The draws below stay inside these ranges and needn't reach their ends.
Inputs may be any that keep to these rules, and one draw needn't show every extreme that they name: `routes`: A token's 2 experts differ. Among the tokens of one index of ep (aligned blocks of 256 rows), no expert is named by more than 32 tokens, a bound that some block reaches.
All inputs are finite; a program needn't handle non-finite values.
Results may differ from the reference program's by a relative error of at most 0.017.
Values may be sent and summed in bfloat16 or wider, within the bound.
No kernel may reach another device: no remote copies, remote signals or barrier semaphores. Data moves between devices by JAX's collectives and lax.ppermute only.
A program may use at most 64 MiB of HBM per device.

```python
import math
import jax
import jax.numpy as jnp
import numpy as np
from jax import lax

D = 2048
FF = 6144
TOPK = 2
TOK_DEV = 256
EXPERTS = 32
CAP = 32
TOKENS = 8192
N_EP = 32
N_TP = 16


def draw_tokens(key, part):
    first, second = jax.random.split(jax.random.fold_in(key, 11))
    scales = 10.0 ** jax.random.uniform(first, (TOKENS, 1), jnp.float32)
    columns = 10.0 ** (jnp.arange(D, dtype=jnp.float32) / (D - 1))
    base = jnp.clip(jax.random.normal(second, (TOKENS, D), jnp.float32), -4.0, 4.0)
    return (base * scales * columns[None, :]).astype(jnp.bfloat16)


def draw_w_down(key, part):
    first = jax.random.fold_in(jax.random.fold_in(key, 23), 0)
    columns = jnp.arange(D, dtype=jnp.float32) / (D - 1)
    scales = 10.0 ** columns
    base = jnp.clip(jax.random.normal(first, (EXPERTS, FF, D), jnp.float32), -4.0, 4.0)
    return (base * scales[None, None, :] * FF ** (-0.5)).astype(jnp.bfloat16)


def steps_of(stream_key, dims, pieces, smallest, largest):
    loudness, own = 1.0, jax.random.fold_in(stream_key, 6)
    for axis_at, blocks in pieces:
        draws = jnp.exp(jax.random.uniform(jax.random.fold_in(own, axis_at), (blocks,), jnp.float32, smallest / len(pieces), largest / len(pieces)))
        loudness = loudness * jnp.repeat(draws, dims[axis_at] // blocks).reshape([-1 if axis == axis_at else 1 for axis in range(len(dims))])
    return loudness


def deal_out(key, own, number, rows, count, top, limit, skew):
    sequence = jax.random.permutation(key, count)
    crowded, common = load_shares(count, rows * top, limit, skew, True), load_shares(count, rows * top, limit, skew, False)
    places = jnp.arange(count)

    def named(sizes, rotation):
        used = int((sizes > 0).sum())
        fixed = max(1, used // 4)
        shifted = fixed + (places - fixed + rotation * (used - fixed)) % max(1, count - fixed)
        return jnp.zeros((count,), jnp.int32).at[sequence[jnp.where(places < fixed, places, shifted)]].set(jnp.asarray(sizes, jnp.int32))

    sizes = jnp.where(number % 4 == 0, named(crowded, number // 4), named(common, number - number // 4 - 1))
    mixed = jax.random.permutation(jax.random.fold_in(own, 3), count)
    donor, sink = mixed[0:count // 2 * 2:2], mixed[1:count // 2 * 2:2]
    slack = jnp.minimum(sizes[donor] - 1, limit - sizes[sink]) // 2
    slack = jnp.where((donor == sequence[0]) | (sink == sequence[0]) | (sizes[sink] == 0), 0, jnp.maximum(slack, 0))
    shifted = jax.random.randint(jax.random.fold_in(own, 4), (count // 2,), 0, 1 << 20) % (slack + 1)
    sizes = sizes.at[donor].add(-shifted).at[sink].add(shifted)
    labels = jnp.searchsorted(jnp.cumsum(sizes), jnp.arange(rows * top), side="right").astype(jnp.int32)
    grid = labels.reshape(top, rows).T
    grid = grid[jax.random.permutation(jax.random.fold_in(own, 1), rows)]
    rotation = jax.random.randint(jax.random.fold_in(own, 2), (rows, 1), 0, top)
    return jnp.take_along_axis(grid, (jnp.arange(top)[None, :] + rotation) % top, axis=1)


def load_shares(count, total, limit, slope, full):
    portions = [(1 << 20) // math.isqrt(rank ** slope) + 1 for rank in range(1, count + 1)]
    largest = limit if full else min(limit, max(-(-total // count), total * portions[0] // sum(portions)))
    least = 1 if total - largest >= count - 1 else 0
    given, spare = [largest] + [least] * (count - 1), total - largest - least * (count - 1)
    while spare > 0:
        free = [i for i in range(1, count) if given[i] < largest] or [i for i in range(1, count) if given[i] < limit]
        mass, budget = sum([portions[i] for i in free]), spare
        for i in free:
            extra = min(limit - given[i], max(1, budget * portions[i] // mass), spare)
            given[i] = given[i] + extra
            spare = spare - extra
    return np.array(given)


def scatter_about(key, dims, spread, limit, pieces=(), kind=jnp.bfloat16):
    drawn = spread * jax.random.normal(key, dims, jnp.float32)
    if pieces:
        drawn = drawn * steps_of(key, dims, pieces, -0.22, 0.18)
    return jnp.clip(drawn, -limit, limit).astype(kind)


def setup_inputs(seed: int = 0) -> dict:
    streams_of = jax.random.split(jax.random.key(seed), 9)
    tokens = draw_tokens(jax.random.fold_in(streams_of[8], 71), 0)
    norm_gain = jnp.clip(1.0 + 0.18 * jax.random.normal(streams_of[1], (D,), jnp.float32), 0.099609375, 1.8984375).astype(jnp.bfloat16)
    w_gate = scatter_about(streams_of[2], (EXPERTS, D, FF), D ** -0.5, 0.125, ((0, 32), (2, 16)))
    w_up = scatter_about(streams_of[3], (EXPERTS, D, FF), D ** -0.5, 0.125, ((0, 32), (2, 16)))
    w_down = draw_w_down(jax.random.fold_in(streams_of[8], 71), 0)
    routes_keys = jax.random.split(jax.random.fold_in(streams_of[5], 1), TOKENS // TOK_DEV)
    routes_turns = jax.random.permutation(jax.random.fold_in(streams_of[5], 3), TOKENS // TOK_DEV)
    routes = jax.vmap(lambda own, number: deal_out(jax.random.fold_in(streams_of[5], 2), own, number, TOK_DEV, EXPERTS, TOPK, CAP, 2))(routes_keys, routes_turns).reshape((TOKENS, TOPK))
    route_weights = jnp.clip(0.1 + 0.9 * jax.random.uniform(streams_of[6], (TOKENS, TOPK), jnp.float32) ** steps_of(streams_of[6], (TOKENS, TOPK), ((0, 32),), -0.2, 0.2), 0.1, 1.0)
    final_gain = jnp.clip(1.0 + 0.18 * jax.random.normal(streams_of[7], (D,), jnp.float32), 0.099609375, 1.8984375).astype(jnp.bfloat16)
    return {"tokens": tokens, "norm_gain": norm_gain, "w_gate": w_gate, "w_up": w_up, "w_down": w_down, "routes": routes, "route_weights": route_weights, "final_gain": final_gain}


EPS = 1e-06

def reference(tokens, norm_gain, w_gate, w_up, w_down, routes, route_weights, final_gain):
    wide = tokens.astype(jnp.float32)
    scale = lax.rsqrt(lax.optimization_barrier(jnp.mean(wide * wide, axis=1, keepdims=True)) + EPS)
    normed = (wide * scale * norm_gain.astype(jnp.float32)[None, :]).astype(jnp.bfloat16)
    groups = routes.reshape(N_EP, TOK_DEV * TOPK)
    onehot = (groups[:, :, None] == jnp.arange(EXPERTS, dtype=jnp.int32)[None, None, :]).astype(jnp.int32)
    before = jnp.cumsum(onehot, axis=1) - onehot
    slot = lax.optimization_barrier(jnp.sum(before * onehot, axis=2)).astype(jnp.int32)
    source = jnp.broadcast_to(jnp.arange(N_EP, dtype=jnp.int32)[:, None], groups.shape)
    token_ids = jnp.repeat(jnp.arange(TOKENS, dtype=jnp.int32), TOPK).reshape(N_EP, TOK_DEV * TOPK)
    buffer = jnp.zeros((EXPERTS, N_EP, CAP, D), jnp.bfloat16)
    buffer = buffer.at[groups, source, slot].set(normed[token_ids])

    def one_expert(args):
        rows, gate_w, up_w, down_w = args
        rows = rows.reshape(N_EP * CAP, D).astype(jnp.float32)
        gate = jnp.dot(rows, gate_w.astype(jnp.float32), preferred_element_type=jnp.float32)
        up = jnp.dot(rows, up_w.astype(jnp.float32), preferred_element_type=jnp.float32)
        hidden = (jax.nn.silu(gate) * up).astype(jnp.bfloat16)
        blocks = hidden.reshape(N_EP * CAP, N_TP, FF // N_TP).astype(jnp.float32)
        down_blocks = down_w.reshape(N_TP, FF // N_TP, D).astype(jnp.float32)
        parts = jnp.einsum('rbf,bfd->brd', blocks, down_blocks).astype(jnp.bfloat16)
        return lax.optimization_barrier(jnp.sum(parts.astype(jnp.float32), axis=0)).astype(jnp.bfloat16)
    results = lax.map(one_expert, (buffer, w_gate, w_up, w_down))
    results = results.reshape(EXPERTS, N_EP, CAP, D)
    picked = results[groups, source, slot].reshape(TOKENS, TOPK, D)
    combined = jnp.einsum('tkd,tk->td', picked.astype(jnp.float32), route_weights)
    final_scale = lax.rsqrt(lax.optimization_barrier(jnp.mean(combined * combined, axis=1, keepdims=True)) + EPS)
    return (combined * final_scale * final_gain.astype(jnp.float32)[None, :]).astype(jnp.bfloat16)
```

```python
import functools

import jax
import jax.numpy as jnp
from jax import lax
from jax.experimental import pallas as pl
from jax.experimental.pallas import tpu as pltpu
from jax.sharding import Mesh, PartitionSpec as P

EPS = 1e-06
F32 = jnp.float32
BF16 = jnp.bfloat16
GAIN_ROWS = 16


def from_ahead(v, axis, step):
    n = lax.axis_size(axis)
    return lax.ppermute(v, axis, [(i, (i - step) % n) for i in range(n)])


def to_ahead(v, axis, step):
    n = lax.axis_size(axis)
    return lax.ppermute(v, axis, [(i, (i + step) % n) for i in range(n)])


def pack_kernel(pos, routes, weights, tokens, near, far, table):
    tok = tokens.shape[0]
    half = near.shape[0]
    experts = 2 * lax.axis_size("z")
    cap = half // (experts // 2)
    e0 = routes[0:1, :]
    e1 = routes[1:2, :]
    lanes = lax.broadcasted_iota(jnp.int32, (experts, tok), 0)
    hot0 = lanes == e0
    hot1 = lanes == e1
    hot = (hot0 | hot1).astype(F32).astype(BF16)
    row = lax.broadcasted_iota(jnp.int32, (tok, tok), 0)
    col = lax.broadcasted_iota(jnp.int32, (tok, tok), 1)
    earlier = (row < col).astype(F32).astype(BF16)
    before = jnp.dot(hot, earlier, preferred_element_type=F32)

    def place(e, mine):
        slot = jnp.sum(jnp.where(mine, before, 0.0), axis=0, keepdims=True)
        other = jnp.bitwise_xor(jnp.bitwise_and(e, 1), pos[0])
        return other * half + (e >> 1) * cap + slot.astype(jnp.int32)

    t0 = place(e0, hot0)
    t1 = place(e1, hot1)
    for at, out in ((0, near), (half, far)):
        rows = lax.broadcasted_iota(jnp.int32, (half, tok), 0) + at
        put = ((rows == t0) | (rows == t1)).astype(F32).astype(BF16)
        out[...] = jnp.dot(put, tokens[...], preferred_element_type=F32).astype(BF16)
    stack = jnp.concatenate(
        [t0.astype(F32), t1.astype(F32), weights[...], jnp.zeros((4, tok), F32)], axis=0
    )
    table[...] = stack.T


def pack(c, routes, weights, tokens):
    tok, share = tokens.shape
    half = lax.axis_size("z") * 32
    vmem = pl.BlockSpec(memory_space=pltpu.VMEM)
    return pl.pallas_call(
        pack_kernel,
        out_shape=(
            jax.ShapeDtypeStruct((half, share), BF16),
            jax.ShapeDtypeStruct((half, share), BF16),
            jax.ShapeDtypeStruct((tok, 8), F32),
        ),
        in_specs=[pl.BlockSpec(memory_space=pltpu.SMEM), vmem, vmem, vmem],
        out_specs=(vmem, vmem, vmem),
        name="pack",
    )(c, routes, weights, tokens)


def expert_kernel(first, rows, *refs):
    pos, wg, wu, wd = refs[:4]
    refs = refs[4:]
    if not first:
        gain_in = refs[0]
        refs = refs[1:]
    pieces = (refs[0:4], refs[4:8])
    outs = (refs[8:12], refs[12:16])
    refs = refs[16:]
    if first:
        gain_out = refs[0]
        refs = refs[1:]
    x, g_s, u_s, d_s, gain_s, sems, gsem = refs
    y = pos[0]
    xx = pos[1]
    nsem = 0
    xcopies = ([], [])
    gcopies = []
    for h in range(2):
        for a in range(4):
            for b in range(4):
                sy, sx = (a, b) if h == 0 else (b, a)
                blk = sy * 4 + sx
                cp = pltpu.make_async_copy(
                    pieces[h][a].at[b, pl.ds(0, rows), :],
                    x.at[pl.ds(h * rows, rows), pl.ds(blk * 128, 128)],
                    sems.at[nsem],
                )
                nsem += 1
                cp.start()
                xcopies[h].append(cp)
                if first and h == 0:
                    cp = pltpu.make_async_copy(
                        pieces[h][a].at[b, pl.ds(rows, GAIN_ROWS), :],
                        gain_s.at[:, pl.ds(blk * 128, 128)],
                        gsem.at[blk],
                    )
                    cp.start()
                    gcopies.append(cp)
    wcopies = []
    for sy in range(4):
        for sx in range(4):
            blk = sy * 4 + sx
            nat = lax.rem(y + sy, 4) * 4 + lax.rem(xx + sx, 4)
            at = pl.multiple_of(nat * 128, 128)
            for src, dst in (
                (wg.at[pl.ds(at, 128), :], g_s.at[pl.ds(blk * 128, 128), :]),
                (wu.at[pl.ds(at, 128), :], u_s.at[pl.ds(blk * 128, 128), :]),
                (wd.at[:, pl.ds(at, 128)], d_s.at[:, pl.ds(blk * 128, 128)]),
            ):
                cp = pltpu.make_async_copy(src, dst, sems.at[nsem])
                nsem += 1
                cp.start()
                wcopies.append(cp)
    for cp in gcopies:
        cp.wait()
    if first:
        gain_out[...] = gain_s[...]
        gain = gain_s[0:1, :].astype(F32)
    else:
        gain = gain_in[0:1, :].astype(F32)
    width = x.shape[1]
    for h in range(2):
        for cp in xcopies[h]:
            cp.wait()

        def norm(i, _):
            at = pl.multiple_of(h * rows + i * 32, 32)
            v = x[pl.ds(at, 32), :].astype(F32)
            scale = lax.rsqrt(jnp.sum(v * v, axis=1, keepdims=True) * (1.0 / width) + EPS)
            x[pl.ds(at, 32), :] = (v * scale * gain).astype(BF16)
            return 0

        lax.fori_loop(0, rows // 32, norm, 0)
        if h == 0:
            for cp in wcopies:
                cp.wait()
        v = x[pl.ds(h * rows, rows), :]
        gate = jnp.dot(v, g_s[...], preferred_element_type=F32)
        up = jnp.dot(v, u_s[...], preferred_element_type=F32)
        hidden = (gate * up / (1.0 + jnp.exp(-gate))).astype(BF16)
        for a in range(4):
            if h == 0:
                res = jnp.dot(
                    hidden, d_s[:, a * 512 : (a + 1) * 512], preferred_element_type=F32
                ).astype(BF16)
                for b in range(4):
                    outs[0][a][b] = res[:, b * 128 : (b + 1) * 128]
            else:
                res = jnp.dot(
                    hidden, d_s[:, a * 512 : (a + 1) * 512], preferred_element_type=F32
                ).astype(BF16)
                for b in range(4):
                    outs[1][b][a] = res[:, b * 128 : (b + 1) * 128]


def expert(first, pos, wg, wu, wd, gain, a_pieces, b_pieces):
    rows = b_pieces[0].shape[1]
    width, units = wg.shape
    hbm = pl.BlockSpec(memory_space=pl.ANY)
    vmem = pl.BlockSpec(memory_space=pltpu.VMEM)
    piece = jax.ShapeDtypeStruct((4, rows, 128), BF16)
    outs = [piece] * 8
    if first:
        outs.append(jax.ShapeDtypeStruct((GAIN_ROWS, width), BF16))
    extra = [] if first else [gain]
    res = pl.pallas_call(
        functools.partial(expert_kernel, first, rows),
        out_shape=tuple(outs),
        in_specs=[pl.BlockSpec(memory_space=pltpu.SMEM)]
        + [hbm] * 3
        + [vmem] * len(extra)
        + [hbm] * 8,
        out_specs=tuple([vmem] * len(outs)),
        scratch_shapes=[
            pltpu.VMEM((2 * rows, width), BF16),
            pltpu.VMEM((width, units), BF16),
            pltpu.VMEM((width, units), BF16),
            pltpu.VMEM((units, width), BF16),
            pltpu.VMEM((GAIN_ROWS, width), BF16),
            pltpu.SemaphoreType.DMA((80,)),
            pltpu.SemaphoreType.DMA((16,)),
        ],
        name="expert_first" if first else "expert_rest",
    )(pos, wg, wu, wd, *extra, *a_pieces, *b_pieces)
    return res[0:4], res[4:8], (res[8] if first else gain)


def combine_kernel(table, near, far, combined, squares):
    tok = table.shape[0]
    half = near.shape[0]
    cols = lax.broadcasted_iota(jnp.int32, (tok, half), 1)
    total = None
    for k in range(2):
        target = table[:, k : k + 1].astype(jnp.int32)
        got = None
        for at, src in ((0, near), (half, far)):
            pick = (cols + at == target).astype(F32).astype(BF16)
            part = jnp.dot(pick, src[...], preferred_element_type=F32)
            got = part if got is None else got + part
        term = got * table[:, 2 + k : 3 + k]
        total = term if total is None else total + term
    combined[...] = total
    squares[...] = jnp.sum((total * total).T, axis=0, keepdims=True)


def combine(table, near, far):
    tok = table.shape[0]
    share = near.shape[1]
    vmem = pl.BlockSpec(memory_space=pltpu.VMEM)
    return pl.pallas_call(
        combine_kernel,
        out_shape=(
            jax.ShapeDtypeStruct((tok, share), F32),
            jax.ShapeDtypeStruct((1, tok), F32),
        ),
        in_specs=[vmem] * 3,
        out_specs=(vmem, vmem),
        name="combine",
    )(table, near, far)


def spread(v_a, v_b):
    a = jnp.stack([v_a] + [from_ahead(v_a, "x", s) for s in (1, 2, 3)])
    b = jnp.stack([v_b] + [from_ahead(v_b, "y", s) for s in (1, 2, 3)])
    a_all = [a] + [from_ahead(a, "y", s) for s in (1, 2, 3)]
    b_all = [b] + [from_ahead(b, "x", s) for s in (1, 2, 3)]
    return a_all, b_all


def total_of(parts):
    total = parts[0].astype(F32)
    for p in parts[1:]:
        total = total + p.astype(F32)
    return total.astype(BF16)


def shrink(a_out, b_out):
    a = total_of([a_out[0]] + [to_ahead(a_out[s], "y", s) for s in (1, 2, 3)])
    b = total_of([b_out[0]] + [to_ahead(b_out[s], "x", s) for s in (1, 2, 3)])
    a = total_of([a[0]] + [to_ahead(a[s], "x", s) for s in (1, 2, 3)])
    b = total_of([b[0]] + [to_ahead(b[s], "y", s) for s in (1, 2, 3)])
    return jnp.concatenate([a, b], axis=0)


def over_z(v):
    n = lax.axis_size("z")
    cut = v.reshape(n, v.shape[0] // n, v.shape[1])
    return lax.all_to_all(cut, "z", split_axis=0, concat_axis=0, tiled=True).reshape(v.shape)


def local(tokens, norm_gain, w_gate, w_up, w_down, routes, route_weights, final_gain):
    tok, share = tokens.shape
    width = share * 16
    c = lax.axis_index("c").astype(jnp.int32)
    pos = jnp.stack([lax.axis_index("y"), lax.axis_index("x")]).astype(jnp.int32)
    near, far, table = pack(c.reshape(1), routes.T, route_weights.T, tokens)
    far = to_ahead(far, "c", 1)
    near = over_z(near)
    far = over_z(far)
    half = near.shape[0] // 2
    gain_rows = jnp.broadcast_to(norm_gain[None, :], (GAIN_ROWS, share))
    a0, b0 = spread(jnp.concatenate([near[:half], gain_rows], axis=0), near[half:])
    a1, b1 = spread(far[:half], far[half:])
    ao, bo, gain = expert(True, pos, w_gate[0], w_up[0], w_down[0], None, a0, b0)
    near = over_z(shrink(ao, bo))
    ao, bo, _ = expert(False, pos, w_gate[0], w_up[0], w_down[0], gain, a1, b1)
    far = over_z(shrink(ao, bo))
    far = to_ahead(far, "c", 1)
    combined, squares = combine(table, near, far)
    copies = jnp.broadcast_to(squares, (16, tok))
    total = lax.all_to_all(copies, ("y", "x"), 0, 0, tiled=True).sum(axis=0)
    scale = lax.rsqrt(total / width + EPS)
    return (combined * scale[:, None] * final_gain.astype(F32)[None, :]).astype(BF16)


def solution(mesh):
    fine = Mesh(mesh.devices.reshape(16, 2, 4, 4), ("z", "c", "y", "x"))
    ep = ("z", "c")
    tp = ("y", "x")
    in_specs = (
        P(ep, tp),
        P(tp),
        P(ep, None, tp),
        P(ep, None, tp),
        P(ep, tp, None),
        P(ep, None),
        P(ep, None),
        P(tp),
    )
    return jax.shard_map(
        local, mesh=fine, in_specs=in_specs, out_specs=P(ep, tp), check_vma=False
    )
```

```python
import functools

import jax
import jax.numpy as jnp
from jax import lax
from jax.experimental import pallas as pl
from jax.experimental.pallas import tpu as pltpu
from jax.sharding import Mesh, PartitionSpec as P


EPS = 1e-06
F32 = jnp.float32
BF16 = jnp.bfloat16
GAIN_ROWS = 16


def pack_kernel(pos, routes, weights, tokens, near, far, table):
    tok = tokens.shape[0]
    half = near.shape[0]
    experts = 2 * lax.axis_size("z")
    cap = half // (experts // 2)
    e0 = routes[0:1, :]
    e1 = routes[1:2, :]
    lanes = lax.broadcasted_iota(jnp.int32, (experts, tok), 0)
    hot0 = lanes == e0
    hot1 = lanes == e1
    hot = (hot0 | hot1).astype(F32).astype(BF16)
    row = lax.broadcasted_iota(jnp.int32, (tok, tok), 0)
    col = lax.broadcasted_iota(jnp.int32, (tok, tok), 1)
    earlier = (row < col).astype(F32).astype(BF16)
    before = jnp.dot(hot, earlier, preferred_element_type=F32)

    def place(e, mine):
        slot = jnp.sum(jnp.where(mine, before, 0.0), axis=0, keepdims=True)
        other = jnp.bitwise_xor(jnp.bitwise_and(e, 1), pos[0])
        return other * half + (e >> 1) * cap + slot.astype(jnp.int32)

    t0 = place(e0, hot0)
    t1 = place(e1, hot1)
    for at, out in ((0, near), (half, far)):
        rows = lax.broadcasted_iota(jnp.int32, (half, tok), 0) + at
        put = ((rows == t0) | (rows == t1)).astype(F32).astype(BF16)
        out[...] = jnp.dot(put, tokens[...], preferred_element_type=F32).astype(BF16)
    stack = jnp.concatenate(
        [t0.astype(F32), t1.astype(F32), weights[...], jnp.zeros((4, tok), F32)], axis=0
    )
    table[...] = stack.T


def pack(c, routes, weights, tokens):
    tok, share = tokens.shape
    half = lax.axis_size("z") * 32
    vmem = pl.BlockSpec(memory_space=pltpu.VMEM)
    return pl.pallas_call(
        pack_kernel,
        out_shape=(
            jax.ShapeDtypeStruct((half, share), BF16),
            jax.ShapeDtypeStruct((half, share), BF16),
            jax.ShapeDtypeStruct((tok, 8), F32),
        ),
        in_specs=[pl.BlockSpec(memory_space=pltpu.SMEM), vmem, vmem, vmem],
        out_specs=(vmem, vmem, vmem),
        name="pack",
    )(c, routes, weights, tokens)


def expert_kernel(first, rows, *refs):
    if first:
        xs, wg, wu, wd, out, gain_out = refs[:6]
        refs = refs[6:]
    else:
        pos = refs[0]
        xs = refs[1:5]
        wg, wu, wd, gain_in = refs[5:9]
        outs = refs[9:13]
        refs = refs[13:]
    raw, gain_s, xn, g_s, u_s, d_s, stage, sems, osems = refs

    def fetch(n, src, dst):
        cp = pltpu.make_async_copy(src, dst, sems.at[n])
        cp.start()
        return cp

    if first:
        gain_cp = fetch(0, xs.at[:, :, pl.ds(rows, GAIN_ROWS), :], gain_s)
        x_cp = [fetch(1, xs.at[:, :, pl.ds(0, rows), :], raw)]
    else:
        gain_cp = fetch(0, gain_in, gain_s)
        x_cp = [fetch(1 + s, xs[s], raw.at[lax.rem(pos[0] + s, 4)]) for s in range(4)]
    g_cp = fetch(5, wg, g_s)
    u_cp = fetch(6, wu, u_s)
    d_cp = fetch(7, wd, d_s)
    gain_cp.wait()
    copies = []
    if first:
        cp = pltpu.make_async_copy(gain_s, gain_out, osems.at[4])
        cp.start()
        copies.append(cp)
    width = xn.shape[1]
    step = 32
    for cp in x_cp:
        cp.wait()

    def norm(i, _):
        at = pl.multiple_of(i * step, step)
        acc = jnp.zeros((step, 128), F32)
        vals = []
        for j in range(16):
            a, b = (j // 4, j % 4) if first else (j % 4, j // 4)
            v = raw[a, b, pl.ds(at, step), :].astype(F32)
            vals.append(v)
            acc = acc + v * v
        scale = lax.rsqrt(jnp.sum(acc, axis=1, keepdims=True) * (1.0 / width) + EPS)
        for j in range(16):
            gain = gain_s[j // 4, j % 4, 0:1, :].astype(F32)
            xn[pl.ds(at, step), j * 128 : (j + 1) * 128] = (vals[j] * scale * gain).astype(BF16)
        return 0

    lax.fori_loop(0, rows // step, norm, 0)
    g_cp.wait()
    gate = jnp.dot(xn[...], g_s[...], preferred_element_type=F32)
    u_cp.wait()
    up = jnp.dot(xn[...], u_s[...], preferred_element_type=F32)
    hidden = (gate * up / (1.0 + jnp.exp(-gate))).astype(BF16)
    d_cp.wait()
    for y in range(4):
        res = jnp.dot(
            hidden, d_s[:, y * 512 : (y + 1) * 512], preferred_element_type=F32
        ).astype(BF16)
        for x in range(4):
            part = res[:, x * 128 : (x + 1) * 128]
            if first:
                stage[y, x] = part
            else:
                stage[x, y] = part
        if first:
            cp = pltpu.make_async_copy(stage.at[y], out.at[y], osems.at[y])
            cp.start()
            copies.append(cp)
    if not first:
        for s in range(4):
            cp = pltpu.make_async_copy(stage.at[lax.rem(pos[0] + s, 4)], outs[s], osems.at[s])
            cp.start()
            copies.append(cp)
    for cp in copies:
        cp.wait()


def expert(first, pos, xs, weights, gain):
    rows = 512
    width, units = weights[0].shape
    hbm = pl.BlockSpec(memory_space=pltpu.HBM)
    gain_type = jax.ShapeDtypeStruct((4, 4, GAIN_ROWS, 128), BF16)
    if first:
        args = (xs, *weights)
        in_specs = [hbm] * 4
        outs = (jax.ShapeDtypeStruct((4, 4, rows, 128), BF16), gain_type)
    else:
        args = (pos, *xs, *weights, gain)
        in_specs = [pl.BlockSpec(memory_space=pltpu.SMEM)] + [hbm] * 8
        outs = tuple([jax.ShapeDtypeStruct((4, rows, 128), BF16)] * 4)
    return pl.pallas_call(
        functools.partial(expert_kernel, first, rows),
        out_shape=outs,
        in_specs=in_specs,
        out_specs=tuple([hbm] * len(outs)),
        scratch_shapes=[
            pltpu.VMEM((4, 4, rows, 128), BF16),
            pltpu.VMEM((4, 4, GAIN_ROWS, 128), BF16),
            pltpu.VMEM((rows, width), BF16),
            pltpu.VMEM((width, units), BF16),
            pltpu.VMEM((width, units), BF16),
            pltpu.VMEM((units, width), BF16),
            pltpu.VMEM((4, 4, rows, 128), BF16),
            pltpu.SemaphoreType.DMA((8,)),
            pltpu.SemaphoreType.DMA((5,)),
        ],
        compiler_params=pltpu.CompilerParams(vmem_limit_bytes=63 * 1024 * 1024),
        name="expert_a" if first else "expert_b",
    )(*args)


def combine_kernel(table, near, far, combined, squares):
    tok = table.shape[0]
    half = near.shape[0]
    cols = lax.broadcasted_iota(jnp.int32, (tok, half), 1)
    total = None
    for k in range(2):
        target = table[:, k : k + 1].astype(jnp.int32)
        got = None
        for at, src in ((0, near), (half, far)):
            pick = (cols + at == target).astype(F32).astype(BF16)
            part = jnp.dot(pick, src[...], preferred_element_type=F32)
            got = part if got is None else got + part
        term = got * table[:, 2 + k : 3 + k]
        total = term if total is None else total + term
    combined[...] = total
    squares[...] = jnp.sum((total * total).T, axis=0, keepdims=True)


def combine(table, near, far):
    tok = table.shape[0]
    share = near.shape[1]
    vmem = pl.BlockSpec(memory_space=pltpu.VMEM)
    return pl.pallas_call(
        combine_kernel,
        out_shape=(
            jax.ShapeDtypeStruct((tok, share), F32),
            jax.ShapeDtypeStruct((1, tok), F32),
        ),
        in_specs=[vmem] * 3,
        out_specs=(vmem, vmem),
        name="combine",
    )(table, near, far)


def exchange(v, axis):
    return lax.all_to_all(v, axis, split_axis=0, concat_axis=0, tiled=True)


def total_of(parts):
    total = parts[0].astype(F32)
    for p in parts[1:]:
        total = total + p.astype(F32)
    return total.astype(BF16)


def over_z(v):
    n = lax.axis_size("z")
    return exchange(v.reshape(n, v.shape[0] // n, v.shape[1]), "z").reshape(v.shape)


def shift(v, axis, step):
    n = lax.axis_size(axis)
    return lax.ppermute(v, axis, [(i, (i + step) % n) for i in range(n)])


def cross(v, step):
    pairs = [(c * 4 + y, (1 - c) * 4 + (y + step) % 4) for c in range(2) for y in range(4)]
    return lax.ppermute(v, ("c", "y"), pairs)


def pick(v, i):
    return lax.dynamic_index_in_dim(v, i, 0, keepdims=False, allow_negative_indices=False)


def local(tokens, norm_gain, w_gate, w_up, w_down, routes, route_weights, final_gain):
    tok, share = tokens.shape
    width = share * 16
    c = lax.axis_index("c").astype(jnp.int32)
    pos = lax.axis_index("x").astype(jnp.int32).reshape(1)
    near, far, table = pack(c.reshape(1), routes.T, route_weights.T, tokens)
    weights = (w_gate[0], w_up[0], w_down[0])
    near = over_z(near)
    far = over_z(shift(far, "c", 1))
    gain_rows = jnp.broadcast_to(norm_gain[None, :], (GAIN_ROWS, share))
    a = lax.all_gather(jnp.concatenate([near, gain_rows], axis=0), "x")
    a, far = lax.optimization_barrier((a, far))
    a = exchange(jnp.broadcast_to(a[None], (4, *a.shape)), "y")
    b = lax.all_gather(far, "y")
    b = [b] + [shift(b, "x", -s) for s in (1, 2, 3)]
    a, gain = expert(True, None, a, weights, None)
    b = expert(False, pos, b, weights, gain)
    a = exchange(a, "y").astype(F32).sum(axis=0).astype(BF16)
    a = exchange(a, "x").astype(F32).sum(axis=0).astype(BF16)
    near = over_z(a)
    b = total_of([b[0]] + [shift(b[s], "x", s) for s in (1, 2, 3)])
    y = lax.axis_index("y").astype(jnp.int32)
    b = total_of([cross(pick(b, jnp.bitwise_and(y + s, 3)), s) for s in range(4)])
    far = over_z(b)
    combined, squares = combine(table, near, far)
    copies = jnp.broadcast_to(squares, (16, tok))
    total = exchange(copies, ("y", "x")).sum(axis=0)
    scale = lax.rsqrt(total / width + EPS)
    return (combined * scale[:, None] * final_gain.astype(F32)[None, :]).astype(BF16)


def solution(mesh):
    fine = Mesh(mesh.devices.reshape(16, 2, 4, 4), ("z", "c", "y", "x"))
    ep = ("z", "c")
    tp = ("y", "x")
    in_specs = (
        P(ep, tp),
        P(tp),
        P(ep, None, tp),
        P(ep, None, tp),
        P(ep, tp, None),
        P(ep, None),
        P(ep, None),
        P(tp),
    )
    return jax.shard_map(
        local, mesh=fine, in_specs=in_specs, out_specs=P(ep, tp), check_vma=False
    )
```

```python
import functools

import jax
import jax.numpy as jnp
from jax import lax
from jax.experimental import pallas as pl
from jax.experimental.pallas import tpu as pltpu
from jax.sharding import Mesh, PartitionSpec as P


EPS = 1e-06
F32 = jnp.float32
BF16 = jnp.bfloat16
GAIN_ROWS = 16


def pack_kernel(pos, routes, weights, tokens, near, far, table):
    tok = tokens.shape[0]
    half = near.shape[0]
    experts = 2 * lax.axis_size("z")
    cap = half // (experts // 2)
    e0 = routes[0:1, :]
    e1 = routes[1:2, :]
    lanes = lax.broadcasted_iota(jnp.int32, (experts, tok), 0)
    hot0 = lanes == e0
    hot1 = lanes == e1
    hot = (hot0 | hot1).astype(F32).astype(BF16)
    row = lax.broadcasted_iota(jnp.int32, (tok, tok), 0)
    col = lax.broadcasted_iota(jnp.int32, (tok, tok), 1)
    earlier = (row < col).astype(F32).astype(BF16)
    before = jnp.dot(hot, earlier, preferred_element_type=F32)

    def place(e, mine):
        slot = jnp.sum(jnp.where(mine, before, 0.0), axis=0, keepdims=True)
        other = jnp.bitwise_xor(jnp.bitwise_and(e, 1), pos[0])
        return other * half + (e >> 1) * cap + slot.astype(jnp.int32)

    t0 = place(e0, hot0)
    t1 = place(e1, hot1)
    for at, out in ((0, near), (half, far)):
        rows = lax.broadcasted_iota(jnp.int32, (half, tok), 0) + at
        put = ((rows == t0) | (rows == t1)).astype(F32).astype(BF16)
        out[...] = jnp.dot(put, tokens[...], preferred_element_type=F32).astype(BF16)
    stack = jnp.concatenate(
        [t0.astype(F32), t1.astype(F32), weights[...], jnp.zeros((4, tok), F32)], axis=0
    )
    table[...] = stack.T


def pack(c, routes, weights, tokens):
    tok, share = tokens.shape
    half = lax.axis_size("z") * 32
    vmem = pl.BlockSpec(memory_space=pltpu.VMEM)
    return pl.pallas_call(
        pack_kernel,
        out_shape=(
            jax.ShapeDtypeStruct((half, share), BF16),
            jax.ShapeDtypeStruct((half, share), BF16),
            jax.ShapeDtypeStruct((tok, 8), F32),
        ),
        in_specs=[pl.BlockSpec(memory_space=pltpu.SMEM), vmem, vmem, vmem],
        out_specs=(vmem, vmem, vmem),
        name="pack",
    )(c, routes, weights, tokens)


def expert_kernel(first, rows, *refs):
    where = refs[0]
    xs = refs[1:5]
    wg, wu, wd = refs[5:8]
    refs = refs[8:]
    if first:
        outs = refs[0:1]
        gain_out = refs[1]
        refs = refs[2:]
    else:
        gain_in = refs[0]
        outs = refs[1:5]
        refs = refs[5:]
    raw, gain_s, xn, g_s, u_s, d_s, stage, sems, osems = refs
    core = where[0]
    at_outer = where[1]

    def block(step, inner):
        outer = jnp.bitwise_and(at_outer + step, 3)
        return jnp.where(core == 0, outer * 4 + inner, inner * 4 + outer)

    def fetch(n, src, dst):
        cp = pltpu.make_async_copy(src, dst, sems.at[n])
        cp.start()
        return cp

    gain_cp = []
    x_cp = []
    for s in range(4):
        for i in range(4):
            n = s * 4 + i
            j = block(s, i)
            x_cp.append(fetch(n, xs[s].at[i, pl.ds(0, rows), :], raw.at[j]))
            if first:
                gain_cp.append(
                    fetch(16 + n, xs[s].at[i, pl.ds(rows, GAIN_ROWS), :], gain_s.at[j])
                )
    if not first:
        gain_cp.append(fetch(16, gain_in, gain_s))
    g_cp = fetch(32, wg, g_s)
    u_cp = fetch(33, wu, u_s)
    d_cp = fetch(34, wd, d_s)
    for cp in gain_cp:
        cp.wait()
    copies = []

    def store(n, src, dst):
        cp = pltpu.make_async_copy(src, dst, osems.at[n])
        cp.start()
        copies.append(cp)

    if first:
        store(16, gain_s, gain_out)
    width = xn.shape[1]
    step = 32
    for cp in x_cp:
        cp.wait()

    def norm(i, _):
        at = pl.multiple_of(i * step, step)
        acc = jnp.zeros((step, 128), F32)
        vals = []
        for j in range(16):
            v = raw[j, pl.ds(at, step), :].astype(F32)
            vals.append(v)
            acc = acc + v * v
        scale = lax.rsqrt(jnp.sum(acc, axis=1, keepdims=True) * (1.0 / width) + EPS)
        for j in range(16):
            gain = gain_s[j, 0:1, :].astype(F32)
            xn[pl.ds(at, step), j * 128 : (j + 1) * 128] = (vals[j] * scale * gain).astype(BF16)
        return 0

    lax.fori_loop(0, rows // step, norm, 0)
    g_cp.wait()
    gate = jnp.dot(xn[...], g_s[...], preferred_element_type=F32)
    u_cp.wait()
    up = jnp.dot(xn[...], u_s[...], preferred_element_type=F32)
    hidden = (gate * up / (1.0 + jnp.exp(-gate))).astype(BF16)
    d_cp.wait()
    for y in range(4):
        res = jnp.dot(
            hidden, d_s[:, y * 512 : (y + 1) * 512], preferred_element_type=F32
        ).astype(BF16)
        for x in range(4):
            stage[y * 4 + x] = res[:, x * 128 : (x + 1) * 128]
            if first:
                outer = jnp.where(core == 0, y, x)
                inner = jnp.where(core == 0, x, y)
                store(y * 4 + x, stage.at[y * 4 + x], outs[0].at[outer, inner])
    if not first:
        for s in range(4):
            for i in range(4):
                store(s * 4 + i, stage.at[block(s, i)], outs[s].at[i])
    for cp in copies:
        cp.wait()


def expert(first, where, xs, weights, gain):
    rows = 512
    width, units = weights[0].shape
    hbm = pl.BlockSpec(memory_space=pltpu.HBM)
    if first:
        args = (where, *xs, *weights)
        outs = (
            jax.ShapeDtypeStruct((4, 4, rows, 128), BF16),
            jax.ShapeDtypeStruct((16, GAIN_ROWS, 128), BF16),
        )
    else:
        args = (where, *xs, *weights, gain)
        outs = tuple([jax.ShapeDtypeStruct((4, rows, 128), BF16)] * 4)
    return pl.pallas_call(
        functools.partial(expert_kernel, first, rows),
        out_shape=outs,
        in_specs=[pl.BlockSpec(memory_space=pltpu.SMEM)] + [hbm] * (len(args) - 1),
        out_specs=tuple([hbm] * len(outs)),
        scratch_shapes=[
            pltpu.VMEM((16, rows, 128), BF16),
            pltpu.VMEM((16, GAIN_ROWS, 128), BF16),
            pltpu.VMEM((rows, width), BF16),
            pltpu.VMEM((width, units), BF16),
            pltpu.VMEM((width, units), BF16),
            pltpu.VMEM((units, width), BF16),
            pltpu.VMEM((16, rows, 128), BF16),
            pltpu.SemaphoreType.DMA((35,)),
            pltpu.SemaphoreType.DMA((17,)),
        ],
        compiler_params=pltpu.CompilerParams(vmem_limit_bytes=63 * 1024 * 1024),
        name="expert_far" if first else "expert_near",
    )(*args)


def combine_kernel(table, near, far, combined, squares):
    tok = table.shape[0]
    half = near.shape[0]
    cols = lax.broadcasted_iota(jnp.int32, (tok, half), 1)
    total = None
    for k in range(2):
        target = table[:, k : k + 1].astype(jnp.int32)
        got = None
        for at, src in ((0, near), (half, far)):
            pick = (cols + at == target).astype(F32).astype(BF16)
            part = jnp.dot(pick, src[...], preferred_element_type=F32)
            got = part if got is None else got + part
        term = got * table[:, 2 + k : 3 + k]
        total = term if total is None else total + term
    combined[...] = total
    squares[...] = jnp.sum((total * total).T, axis=0, keepdims=True)


def combine(table, near, far):
    tok = table.shape[0]
    share = near.shape[1]
    vmem = pl.BlockSpec(memory_space=pltpu.VMEM)
    return pl.pallas_call(
        combine_kernel,
        out_shape=(
            jax.ShapeDtypeStruct((tok, share), F32),
            jax.ShapeDtypeStruct((1, tok), F32),
        ),
        in_specs=[vmem] * 3,
        out_specs=(vmem, vmem),
        name="combine",
    )(table, near, far)


ALL = ("z", "c", "y", "x")


def flat(z, c, y, x):
    return ((z * 2 + c) * 4 + y) * 4 + x


def lines(along_x_for):
    groups = []
    for z in range(16):
        for c in range(2):
            for i in range(4):
                if c == along_x_for:
                    groups.append([flat(z, c, i, x) for x in range(4)])
                else:
                    groups.append([flat(z, c, y, i) for y in range(4)])
    return groups


def exchange(v, axis, groups=None):
    return lax.all_to_all(
        v, axis, split_axis=0, concat_axis=0, tiled=True, axis_index_groups=groups
    )


def inner_exchange(v):
    return exchange(v, ALL, lines(0))


def outer_exchange(v):
    return exchange(v, ALL, lines(1))


def outer_shift(v, step):
    pairs = []
    for z in range(16):
        for y in range(4):
            for x in range(4):
                pairs.append((flat(z, 0, y, x), flat(z, 0, (y + step) % 4, x)))
                pairs.append((flat(z, 1, y, x), flat(z, 1, y, (x + step) % 4)))
    return lax.ppermute(v, ALL, pairs)


def swap(v):
    return lax.ppermute(v, "c", [(0, 1), (1, 0)])


def total_of(parts):
    total = parts[0].astype(F32)
    for p in parts[1:]:
        total = total + p.astype(F32)
    return total.astype(BF16)


def summed(v):
    return v.astype(F32).sum(axis=0).astype(BF16)


def over_z(near, far):
    share = near.shape[1]
    both = jnp.stack([near.reshape(16, -1, share), far.reshape(16, -1, share)], axis=1)
    both = exchange(both, "z")
    return both[:, 0].reshape(near.shape), both[:, 1].reshape(far.shape)


def local(tokens, norm_gain, w_gate, w_up, w_down, routes, route_weights, final_gain):
    tok, share = tokens.shape
    width = share * 16
    c = lax.axis_index("c").astype(jnp.int32)
    y = lax.axis_index("y").astype(jnp.int32)
    x = lax.axis_index("x").astype(jnp.int32)
    where = jnp.stack([c, jnp.where(c == 0, y, x)])
    near, far, table = pack(c.reshape(1), routes.T, route_weights.T, tokens)
    weights = (w_gate[0], w_up[0], w_down[0])
    near, far = over_z(near, swap(far))
    gain_rows = jnp.broadcast_to(norm_gain[None, :], (GAIN_ROWS, share))
    rows = jnp.concatenate([far, gain_rows, near], axis=0)
    rows = inner_exchange(jnp.broadcast_to(rows[None], (4, *rows.shape)))
    first = far.shape[0] + GAIN_ROWS
    far, near = rows[:, :first], rows[:, first:]
    far = [far] + [outer_shift(far, -s) for s in (1, 2, 3)]
    near = [near] + [outer_shift(near, -s) for s in (1, 2, 3)]
    far, gain = expert(True, where, far, weights, None)
    far = summed(outer_exchange(far))
    near = expert(False, where, near, weights, gain)
    near = total_of([near[0]] + [outer_shift(near[s], s) for s in (1, 2, 3)])
    far = swap(summed(inner_exchange(far)))
    near = summed(inner_exchange(near))
    near, far = over_z(near, far)
    combined, squares = combine(table, near, far)
    copies = jnp.broadcast_to(squares, (16, tok))
    total = exchange(copies, ("y", "x")).sum(axis=0)
    scale = lax.rsqrt(total / width + EPS)
    return (combined * scale[:, None] * final_gain.astype(F32)[None, :]).astype(BF16)


def solution(mesh):
    fine = Mesh(mesh.devices.reshape(16, 2, 4, 4), ("z", "c", "y", "x"))
    ep = ("z", "c")
    tp = ("y", "x")
    in_specs = (
        P(ep, tp),
        P(tp),
        P(ep, None, tp),
        P(ep, None, tp),
        P(ep, tp, None),
        P(ep, None),
        P(ep, None),
        P(tp),
    )
    return jax.shard_map(
        local, mesh=fine, in_specs=in_specs, out_specs=P(ep, tp), check_vma=False
    )
```

```python
import functools

import jax
import jax.numpy as jnp
from jax import lax
from jax.experimental import pallas as pl
from jax.experimental.pallas import tpu as pltpu
from jax.sharding import Mesh, PartitionSpec as P


EPS = 1e-06
F32 = jnp.float32
BF16 = jnp.bfloat16
GAIN_ROWS = 16


def pack_kernel(pos, routes, weights, tokens, near, far, table):
    tok = tokens.shape[0]
    half = near.shape[0]
    experts = 2 * lax.axis_size("z")
    cap = half // (experts // 2)
    e0 = routes[0:1, :]
    e1 = routes[1:2, :]
    lanes = lax.broadcasted_iota(jnp.int32, (experts, tok), 0)
    hot0 = lanes == e0
    hot1 = lanes == e1
    hot = (hot0 | hot1).astype(F32).astype(BF16)
    row = lax.broadcasted_iota(jnp.int32, (tok, tok), 0)
    col = lax.broadcasted_iota(jnp.int32, (tok, tok), 1)
    earlier = (row < col).astype(F32).astype(BF16)
    before = jnp.dot(hot, earlier, preferred_element_type=F32)

    def place(e, mine):
        slot = jnp.sum(jnp.where(mine, before, 0.0), axis=0, keepdims=True)
        other = jnp.bitwise_xor(jnp.bitwise_and(e, 1), pos[0])
        return other * half + (e >> 1) * cap + slot.astype(jnp.int32)

    t0 = place(e0, hot0)
    t1 = place(e1, hot1)
    for at, out in ((0, near), (half, far)):
        rows = lax.broadcasted_iota(jnp.int32, (half, tok), 0) + at
        put = ((rows == t0) | (rows == t1)).astype(F32).astype(BF16)
        out[...] = jnp.dot(put, tokens[...], preferred_element_type=F32).astype(BF16)

    def packed(t):
        other = (t >= half).astype(jnp.int32)
        inside = t - other * half
        at_z = inside // cap
        return (at_z * 2 + other) * cap + (inside - at_z * cap)

    t0 = packed(t0)
    t1 = packed(t1)
    stack = jnp.concatenate(
        [t0.astype(F32), t1.astype(F32), weights[...], jnp.zeros((4, tok), F32)], axis=0
    )
    table[...] = stack.T


def pack(c, routes, weights, tokens):
    tok, share = tokens.shape
    half = lax.axis_size("z") * 32
    vmem = pl.BlockSpec(memory_space=pltpu.VMEM)
    return pl.pallas_call(
        pack_kernel,
        out_shape=(
            jax.ShapeDtypeStruct((half, share), BF16),
            jax.ShapeDtypeStruct((half, share), BF16),
            jax.ShapeDtypeStruct((tok, 8), F32),
        ),
        in_specs=[pl.BlockSpec(memory_space=pltpu.SMEM), vmem, vmem, vmem],
        out_specs=(vmem, vmem, vmem),
        name="pack",
    )(c, routes, weights, tokens)


def expert_kernel(first, rows, core_ref, y_ref, x_ref, xs, *refs):
    if first:
        wg, wu, wd, out, gain_out = refs[:5]
        refs = refs[5:]
        outs = [out.at[o] for o in range(4)]
    else:
        more = refs[0:3]
        wg, wu, wd, gain_in = refs[3:7]
        outs = refs[7:11]
        refs = refs[11:]
    raw, gain_s, xn, gu_s, d_s, stage, sems, osems = refs
    core = core_ref[0]
    at_outer = jnp.where(core == 0, y_ref[0], x_ref[0])

    def block(o, inner):
        outer = o if first else jnp.bitwise_and(at_outer + o, 3)
        return jnp.where(core == 0, outer * 4 + inner, inner * 4 + outer)

    def source(o):
        if first:
            return xs.at[o]
        return xs if o == 0 else more[o - 1]

    count = [0]

    def fetch(src, dst):
        cp = pltpu.make_async_copy(src, dst, sems.at[count[0]])
        count[0] += 1
        cp.start()
        return cp

    half = rows // 2
    width = xn.shape[1]
    units = gu_s.shape[1] // 2

    def fetch_rows(at):
        return [
            fetch(source(o).at[i, pl.ds(at, half), :], raw.at[block(o, i), pl.ds(at, half), :])
            for o in range(4)
            for i in range(4)
        ]

    x_cp = [fetch_rows(0)]
    if first:
        gain_cp = [
            fetch(source(o).at[i, pl.ds(rows, GAIN_ROWS), :], gain_s.at[block(o, i)])
            for o in range(4)
            for i in range(4)
        ]
    else:
        gain_cp = [fetch(gain_in, gain_s)]
    w_cp = [fetch(wg, gu_s.at[:, pl.ds(0, units)]), fetch(wu, gu_s.at[:, pl.ds(units, units)])]
    x_cp.append(fetch_rows(half))
    d_cp = [
        fetch(
            wd.at[:, pl.ds(pl.multiple_of(block(o, i) * 128, 128), 128)],
            d_s.at[:, pl.ds((o * 4 + i) * 128, 128)],
        )
        for o in range(4)
        for i in range(4)
    ]
    for cp in gain_cp:
        cp.wait()
    copies = []

    def store(n, src, dst):
        cp = pltpu.make_async_copy(src, dst, osems.at[n])
        cp.start()
        copies.append(cp)

    if first:
        store(4, gain_s, gain_out)
    step = 32

    def norm(i, _):
        at = pl.multiple_of(i * step, step)
        acc = jnp.zeros((step, 128), F32)
        vals = []
        for j in range(16):
            v = raw[j, pl.ds(at, step), :].astype(F32)
            vals.append(v)
            acc = acc + v * v
        scale = lax.rsqrt(jnp.sum(acc, axis=1, keepdims=True) * (1.0 / width) + EPS)
        for j in range(16):
            gain = gain_s[j, 0:1, :].astype(F32)
            xn[pl.ds(at, step), j * 128 : (j + 1) * 128] = (vals[j] * scale * gain).astype(BF16)
        return 0

    steps = half // step
    for h in range(2):
        for cp in x_cp[h]:
            cp.wait()
        lax.fori_loop(h * steps, (h + 1) * steps, norm, 0)
    for cp in w_cp:
        cp.wait()
    both = jnp.dot(xn[...], gu_s[...], preferred_element_type=F32)
    gate = both[:, :units]
    hidden = (gate * both[:, units:] / (1.0 + jnp.exp(-gate))).astype(BF16)
    for cp in d_cp:
        cp.wait()
    for o in range(4):
        res = jnp.dot(
            hidden, d_s[:, o * 512 : (o + 1) * 512], preferred_element_type=F32
        ).astype(BF16)
        for i in range(4):
            stage[o, i] = res[:, i * 128 : (i + 1) * 128]
        store(o, stage.at[o], outs[o])
    for cp in copies:
        cp.wait()


def expert(first, place, xs, weights, gain):
    rows = 512
    width, units = weights[0].shape
    hbm = pl.BlockSpec(memory_space=pltpu.HBM)
    if first:
        args = (*place, xs, *weights)
        outs = (
            jax.ShapeDtypeStruct((4, 4, rows, 128), BF16),
            jax.ShapeDtypeStruct((16, GAIN_ROWS, 128), BF16),
        )
    else:
        args = (*place, *xs, *weights, gain)
        outs = tuple([jax.ShapeDtypeStruct((4, rows, 128), BF16)] * 4)
    return pl.pallas_call(
        functools.partial(expert_kernel, first, rows),
        out_shape=outs,
        in_specs=[pl.BlockSpec(memory_space=pltpu.SMEM)] * 3 + [hbm] * (len(args) - 3),
        out_specs=tuple([hbm] * len(outs)),
        scratch_shapes=[
            pltpu.VMEM((16, rows, 128), BF16),
            pltpu.VMEM((16, GAIN_ROWS, 128), BF16),
            pltpu.VMEM((rows, width), BF16),
            pltpu.VMEM((width, 2 * units), BF16),
            pltpu.VMEM((units, width), BF16),
            pltpu.VMEM((4, 4, rows, 128), BF16),
            pltpu.SemaphoreType.DMA((66,)),
            pltpu.SemaphoreType.DMA((5,)),
        ],
        compiler_params=pltpu.CompilerParams(vmem_limit_bytes=63 * 1024 * 1024),
        name="expert_far" if first else "expert_near",
    )(*args)


def combine_kernel(table, rows, combined, squares):
    tok = table.shape[0]
    count = rows.shape[0]
    cols = lax.broadcasted_iota(jnp.int32, (tok, count), 1)
    total = None
    for k in range(2):
        target = table[:, k : k + 1].astype(jnp.int32)
        pick = (cols == target).astype(F32).astype(BF16)
        got = jnp.dot(pick, rows[...], preferred_element_type=F32)
        term = got * table[:, 2 + k : 3 + k]
        total = term if total is None else total + term
    combined[...] = total
    mine = jnp.sum((total * total).T, axis=0, keepdims=True)
    for i in range(squares.shape[0]):
        squares[i] = mine


def combine(table, rows):
    tok = table.shape[0]
    share = rows.shape[1]
    vmem = pl.BlockSpec(memory_space=pltpu.VMEM)
    return pl.pallas_call(
        combine_kernel,
        out_shape=(
            jax.ShapeDtypeStruct((tok, share), F32),
            jax.ShapeDtypeStruct((16, 1, tok), F32),
        ),
        in_specs=[vmem] * 2,
        out_specs=(vmem, vmem),
        name="combine",
    )(table, rows)


ALL = ("z", "c", "y", "x")


def flat(z, c, y, x):
    return ((z * 2 + c) * 4 + y) * 4 + x


def lines(along_x_for):
    groups = []
    for z in range(16):
        for c in range(2):
            for i in range(4):
                if c == along_x_for:
                    groups.append([flat(z, c, i, x) for x in range(4)])
                else:
                    groups.append([flat(z, c, y, i) for y in range(4)])
    return groups


def exchange(v, axis, groups=None):
    return lax.all_to_all(
        v, axis, split_axis=0, concat_axis=0, tiled=True, axis_index_groups=groups
    )


def inner_exchange(v):
    return exchange(v, ALL, lines(0))


def outer_exchange(v):
    return exchange(v, ALL, lines(1))


def outer_shift(v, step):
    pairs = []
    for z in range(16):
        for y in range(4):
            for x in range(4):
                pairs.append((flat(z, 0, y, x), flat(z, 0, (y + step) % 4, x)))
                pairs.append((flat(z, 1, y, x), flat(z, 1, y, (x + step) % 4)))
    return lax.ppermute(v, ALL, pairs)


def swap(v):
    return lax.ppermute(v, "c", [(0, 1), (1, 0)])


def total_of(parts):
    total = parts[0].astype(F32)
    for p in parts[1:]:
        total = total + p.astype(F32)
    return total.astype(BF16)


def summed(v):
    return v.astype(F32).sum(axis=0).astype(BF16)


def over_z(near, far):
    share = near.shape[1]
    both = jnp.stack([near.reshape(16, -1, share), far.reshape(16, -1, share)], axis=1)
    return exchange(both, "z")


def local(tokens, norm_gain, w_gate, w_up, w_down, routes, route_weights, final_gain):
    _, share = tokens.shape
    width = share * 16
    place = tuple(lax.axis_index(a).astype(jnp.int32).reshape(1) for a in ("c", "y", "x"))
    near, far, table = pack(place[0], routes.T, route_weights.T, tokens)
    weights = (w_gate[0], w_up[0], w_down[0])
    both = over_z(near, swap(far))
    near, far = (both[:, i].reshape(-1, share) for i in range(2))
    gain_rows = jnp.broadcast_to(norm_gain[None, :], (GAIN_ROWS, share))
    rows = jnp.concatenate([far, gain_rows, near], axis=0)
    rows = inner_exchange(jnp.broadcast_to(rows[None], (4, *rows.shape)))
    first = far.shape[0] + GAIN_ROWS
    far = rows[:, :first]
    far = outer_exchange(jnp.broadcast_to(far[None], (4, *far.shape)))
    near = rows[:, first:]
    near = [near] + [outer_shift(near, -s) for s in (1, 2, 3)]
    far, gain = expert(True, place, far, weights, None)
    far = summed(outer_exchange(far))
    near = expert(False, place, near, weights, gain)
    near = total_of([near[0]] + [outer_shift(near[s], s) for s in (1, 2, 3)])
    far = swap(summed(inner_exchange(far)))
    near = summed(inner_exchange(near))
    both = over_z(near, far)
    combined, squares = combine(table, both.reshape(-1, share))
    total = exchange(squares, ("y", "x")).sum(axis=(0, 1))
    scale = lax.rsqrt(total / width + EPS)
    return (combined * scale[:, None] * final_gain.astype(F32)[None, :]).astype(BF16)


def solution(mesh):
    fine = Mesh(mesh.devices.reshape(16, 2, 4, 4), ("z", "c", "y", "x"))
    ep = ("z", "c")
    tp = ("y", "x")
    in_specs = (
        P(ep, tp),
        P(tp),
        P(ep, None, tp),
        P(ep, None, tp),
        P(ep, tp, None),
        P(ep, None),
        P(ep, None),
        P(tp),
    )
    return jax.shard_map(
        local, mesh=fine, in_specs=in_specs, out_specs=P(ep, tp), check_vma=False
    )
```

```python
import functools

import jax
import jax.numpy as jnp
from jax import lax
from jax.experimental import pallas as pl
from jax.experimental.pallas import tpu as pltpu
from jax.sharding import Mesh, PartitionSpec as P


EPS = 1e-06
F32 = jnp.float32
BF16 = jnp.bfloat16
GAIN_ROWS = 16


def pack_kernel(pos, routes, weights, tokens, out, table):
    tok = tokens.shape[0]
    count = out.shape[0]
    experts = 2 * lax.axis_size("z")
    cap = count // experts
    e0 = routes[0:1, :]
    e1 = routes[1:2, :]
    names = lax.broadcasted_iota(jnp.int32, (experts, tok), 0)
    hot0 = names == e0
    hot1 = names == e1
    hot = (hot0 | hot1).astype(F32).astype(BF16)
    row = lax.broadcasted_iota(jnp.int32, (tok, tok), 0)
    col = lax.broadcasted_iota(jnp.int32, (tok, tok), 1)
    earlier = (row < col).astype(F32).astype(BF16)
    before = jnp.dot(hot, earlier, preferred_element_type=F32)

    def place(e, mine):
        slot = jnp.sum(jnp.where(mine, before, 0.0), axis=0, keepdims=True)
        return jnp.bitwise_xor(e, pos[0]) * cap + slot.astype(jnp.int32)

    t0 = place(e0, hot0)
    t1 = place(e1, hot1)
    rows = lax.broadcasted_iota(jnp.int32, (count, tok), 0)
    put = ((rows == t0) | (rows == t1)).astype(F32).astype(BF16)
    out[...] = jnp.dot(put, tokens[...], preferred_element_type=F32).astype(BF16)
    stack = jnp.concatenate(
        [t0.astype(F32), t1.astype(F32), weights[...], jnp.zeros((4, tok), F32)], axis=0
    )
    table[...] = stack.T


def pack(c, routes, weights, tokens):
    tok, share = tokens.shape
    count = 2 * lax.axis_size("z") * 32
    vmem = pl.BlockSpec(memory_space=pltpu.VMEM)
    return pl.pallas_call(
        pack_kernel,
        out_shape=(
            jax.ShapeDtypeStruct((count, share), BF16),
            jax.ShapeDtypeStruct((tok, 8), F32),
        ),
        in_specs=[pl.BlockSpec(memory_space=pltpu.SMEM), vmem, vmem, vmem],
        out_specs=(vmem, vmem),
        name="pack",
    )(c, routes, weights, tokens)


def expert_kernel(first, rows, core_ref, y_ref, x_ref, xs, wg, wu, wd, *refs):
    if first:
        out, gain_out = refs[:2]
    else:
        gain_in, out = refs[:2]
    raw, gain_s, xn, gu_s, d_s, stage, sems, osems = refs[2:]
    core = core_ref[0]
    at_inner = jnp.where(core == 0, x_ref[0], y_ref[0])

    def block(outer, inner):
        return jnp.where(core == 0, outer * 4 + inner, inner * 4 + outer)

    def taken(outer, inner):
        return block(outer, inner if first else jnp.bitwise_and(at_inner + inner, 3))

    count = [0]

    def fetch(src, dst):
        cp = pltpu.make_async_copy(src, dst, sems.at[count[0]])
        count[0] += 1
        cp.start()
        return cp

    half = rows // 2
    width = xn.shape[1]
    units = gu_s.shape[1] // 2

    def fetch_rows(at):
        return [
            fetch(xs.at[o, i, pl.ds(at, half), :], raw.at[taken(o, i), pl.ds(at, half), :])
            for o in range(4)
            for i in range(4)
        ]

    x_cp = [fetch_rows(0)]
    if first:
        gain_cp = [
            fetch(xs.at[o, i, pl.ds(rows, GAIN_ROWS), :], gain_s.at[taken(o, i)])
            for o in range(4)
            for i in range(4)
        ]
    else:
        gain_cp = [fetch(gain_in, gain_s)]
    w_cp = [fetch(wg, gu_s.at[:, pl.ds(0, units)]), fetch(wu, gu_s.at[:, pl.ds(units, units)])]
    x_cp.append(fetch_rows(half))
    d_cp = [
        fetch(
            wd.at[:, pl.ds(pl.multiple_of(block(o, i) * 128, 128), 128)],
            d_s.at[:, pl.ds((o * 4 + i) * 128, 128)],
        )
        for o in range(4)
        for i in range(4)
    ]
    for cp in gain_cp:
        cp.wait()
    copies = []

    def store(n, src, dst):
        cp = pltpu.make_async_copy(src, dst, osems.at[n])
        cp.start()
        copies.append(cp)

    if first:
        store(4, gain_s, gain_out)
    step = 32

    def norm(i, _):
        at = pl.multiple_of(i * step, step)
        acc = jnp.zeros((step, 128), F32)
        vals = []
        for j in range(16):
            v = raw[j, pl.ds(at, step), :].astype(F32)
            vals.append(v)
            acc = acc + v * v
        scale = lax.rsqrt(jnp.sum(acc, axis=1, keepdims=True) * (1.0 / width) + EPS)
        for j in range(16):
            gain = gain_s[j, 0:1, :].astype(F32)
            xn[pl.ds(at, step), j * 128 : (j + 1) * 128] = (vals[j] * scale * gain).astype(BF16)
        return 0

    steps = half // step
    for h in range(2):
        for cp in x_cp[h]:
            cp.wait()
        lax.fori_loop(h * steps, (h + 1) * steps, norm, 0)
    for cp in w_cp:
        cp.wait()
    both = jnp.dot(xn[...], gu_s[...], preferred_element_type=F32)
    gate = both[:, :units]
    hidden = (gate * both[:, units:] / (1.0 + jnp.exp(-gate))).astype(BF16)
    for cp in d_cp:
        cp.wait()
    for o in range(4):
        res = jnp.dot(
            hidden, d_s[:, o * 512 : (o + 1) * 512], preferred_element_type=F32
        ).astype(BF16)
        for i in range(4):
            stage[o, i] = res[:, i * 128 : (i + 1) * 128]
        store(o, stage.at[o], out.at[o])
    for cp in copies:
        cp.wait()


def expert(first, place, xs, weights, gain):
    rows = 512
    width, units = weights[0].shape
    hbm = pl.BlockSpec(memory_space=pltpu.HBM)
    args = (*place, xs, *weights)
    outs = (jax.ShapeDtypeStruct((4, 4, rows, 128), BF16),)
    if first:
        outs = (*outs, jax.ShapeDtypeStruct((16, GAIN_ROWS, 128), BF16))
    else:
        args = (*args, gain)
    return pl.pallas_call(
        functools.partial(expert_kernel, first, rows),
        out_shape=outs,
        in_specs=[pl.BlockSpec(memory_space=pltpu.SMEM)] * 3 + [hbm] * (len(args) - 3),
        out_specs=tuple([hbm] * len(outs)),
        scratch_shapes=[
            pltpu.VMEM((16, rows, 128), BF16),
            pltpu.VMEM((16, GAIN_ROWS, 128), BF16),
            pltpu.VMEM((rows, width), BF16),
            pltpu.VMEM((width, 2 * units), BF16),
            pltpu.VMEM((units, width), BF16),
            pltpu.VMEM((4, 4, rows, 128), BF16),
            pltpu.SemaphoreType.DMA((66,)),
            pltpu.SemaphoreType.DMA((5,)),
        ],
        compiler_params=pltpu.CompilerParams(vmem_limit_bytes=63 * 1024 * 1024),
        name="expert_near" if first else "expert_far",
    )(*args)


def combine_kernel(table, rows, combined, squares):
    tok = table.shape[0]
    count = rows.shape[0]
    cols = lax.broadcasted_iota(jnp.int32, (tok, count), 1)
    total = None
    for k in range(2):
        target = table[:, k : k + 1].astype(jnp.int32)
        pick = (cols == target).astype(F32).astype(BF16)
        got = jnp.dot(pick, rows[...], preferred_element_type=F32)
        term = got * table[:, 2 + k : 3 + k]
        total = term if total is None else total + term
    combined[...] = total
    mine = jnp.sum((total * total).T, axis=0, keepdims=True)
    for i in range(squares.shape[0]):
        squares[i] = mine


def combine(table, rows):
    tok = table.shape[0]
    share = rows.shape[1]
    vmem = pl.BlockSpec(memory_space=pltpu.VMEM)
    return pl.pallas_call(
        combine_kernel,
        out_shape=(
            jax.ShapeDtypeStruct((tok, share), F32),
            jax.ShapeDtypeStruct((16, 1, tok), F32),
        ),
        in_specs=[vmem] * 2,
        out_specs=(vmem, vmem),
        name="combine",
    )(table, rows)


ALL = ("z", "c", "y", "x")


def flat(z, c, y, x):
    return ((z * 2 + c) * 4 + y) * 4 + x


def lines(along_x_for):
    groups = []
    for z in range(16):
        for c in range(2):
            for i in range(4):
                if c == along_x_for:
                    groups.append([flat(z, c, i, x) for x in range(4)])
                else:
                    groups.append([flat(z, c, y, i) for y in range(4)])
    return groups


def exchange(v, axis, groups=None):
    return lax.all_to_all(
        v, axis, split_axis=0, concat_axis=0, tiled=True, axis_index_groups=groups
    )


def inner_exchange(v):
    return exchange(v, ALL, lines(0))


def outer_exchange(v):
    return exchange(v, ALL, lines(1))


def inner_ahead(v, step):
    pairs = []
    for z in range(16):
        for y in range(4):
            for x in range(4):
                pairs.append((flat(z, 0, y, (x + step) % 4), flat(z, 0, y, x)))
                pairs.append((flat(z, 1, (y + step) % 4, x), flat(z, 1, y, x)))
    return lax.ppermute(v, ALL, pairs)


def swap(v):
    return lax.ppermute(v, "c", [(0, 1), (1, 0)])


def total_of(parts):
    total = parts[0].astype(F32)
    for p in parts[1:]:
        total = total + p.astype(F32)
    return total.astype(BF16)


def summed(v):
    return total_of([v[i] for i in range(v.shape[0])])


def copies(v):
    return jnp.broadcast_to(v[None], (4, *v.shape))


def local(tokens, norm_gain, w_gate, w_up, w_down, routes, route_weights, final_gain):
    _, share = tokens.shape
    width = share * 16
    place = tuple(lax.axis_index(a).astype(jnp.int32).reshape(1) for a in ("c", "y", "x"))
    rows, table = pack(place[0], routes.T, route_weights.T, tokens)
    weights = (w_gate[0], w_up[0], w_down[0])
    both = exchange(rows.reshape(16, 2, -1, share), "z")
    near, far = (both[:, i].reshape(-1, share) for i in range(2))
    gain_rows = jnp.broadcast_to(norm_gain[None, :], (GAIN_ROWS, share))
    near = inner_exchange(copies(jnp.concatenate([near, gain_rows], axis=0)))
    far = swap(far)
    near = outer_exchange(copies(near))
    far = jnp.stack([far] + [inner_ahead(far, s) for s in (1, 2, 3)])
    far = outer_exchange(copies(far))
    near, gain = expert(True, place, near, weights, None)
    near = summed(outer_exchange(near))
    far = expert(False, place, far, weights, gain)[0]
    far = summed(outer_exchange(far))
    last = summed(inner_exchange(jnp.concatenate([near, far], axis=1)))
    near = last[: near.shape[1]]
    far = swap(last[near.shape[0] :])
    both = jnp.stack([near.reshape(16, -1, share), far.reshape(16, -1, share)], axis=1)
    combined, squares = combine(table, exchange(both, "z").reshape(-1, share))
    total = exchange(squares, ("y", "x")).sum(axis=(0, 1))
    scale = lax.rsqrt(total / width + EPS)
    return (combined * scale[:, None] * final_gain.astype(F32)[None, :]).astype(BF16)


def solution(mesh):
    fine = Mesh(mesh.devices.reshape(16, 2, 4, 4), ("z", "c", "y", "x"))
    ep = ("z", "c")
    tp = ("y", "x")
    in_specs = (
        P(ep, tp),
        P(tp),
        P(ep, None, tp),
        P(ep, None, tp),
        P(ep, tp, None),
        P(ep, None),
        P(ep, None),
        P(tp),
    )
    return jax.shard_map(
        local, mesh=fine, in_specs=in_specs, out_specs=P(ep, tp), check_vma=False
    )
```

```python
import functools

import jax
import jax.numpy as jnp
from jax import lax
from jax.experimental import pallas as pl
from jax.experimental.pallas import tpu as pltpu
from jax.sharding import Mesh, PartitionSpec as P


EPS = 1e-06
F32 = jnp.float32
BF16 = jnp.bfloat16
GAIN_ROWS = 16


def pack_kernel(pos, routes, weights, tokens, near, far, table):
    tok = tokens.shape[0]
    half = near.shape[0]
    experts = 2 * lax.axis_size("z")
    cap = half // (experts // 2)
    e0 = routes[0:1, :]
    e1 = routes[1:2, :]
    lanes = lax.broadcasted_iota(jnp.int32, (experts, tok), 0)
    hot0 = lanes == e0
    hot1 = lanes == e1
    hot = (hot0 | hot1).astype(F32).astype(BF16)
    row = lax.broadcasted_iota(jnp.int32, (tok, tok), 0)
    col = lax.broadcasted_iota(jnp.int32, (tok, tok), 1)
    earlier = (row < col).astype(F32).astype(BF16)
    before = jnp.dot(hot, earlier, preferred_element_type=F32)

    def place(e, mine):
        slot = jnp.sum(jnp.where(mine, before, 0.0), axis=0, keepdims=True)
        other = jnp.bitwise_xor(jnp.bitwise_and(e, 1), pos[0])
        return other * half + (e >> 1) * cap + slot.astype(jnp.int32)

    t0 = place(e0, hot0)
    t1 = place(e1, hot1)
    for at, out in ((0, near), (half, far)):
        rows = lax.broadcasted_iota(jnp.int32, (half, tok), 0) + at
        put = ((rows == t0) | (rows == t1)).astype(F32).astype(BF16)
        out[...] = jnp.dot(put, tokens[...], preferred_element_type=F32).astype(BF16)

    def packed(t):
        other = (t >= half).astype(jnp.int32)
        inside = t - other * half
        at_z = inside // cap
        return (at_z * 2 + other) * cap + (inside - at_z * cap)

    t0 = packed(t0)
    t1 = packed(t1)
    stack = jnp.concatenate(
        [t0.astype(F32), t1.astype(F32), weights[...], jnp.zeros((4, tok), F32)], axis=0
    )
    table[...] = stack.T


def pack(c, routes, weights, tokens):
    tok, share = tokens.shape
    half = lax.axis_size("z") * 32
    vmem = pl.BlockSpec(memory_space=pltpu.VMEM)
    return pl.pallas_call(
        pack_kernel,
        out_shape=(
            jax.ShapeDtypeStruct((half, share), BF16),
            jax.ShapeDtypeStruct((half, share), BF16),
            jax.ShapeDtypeStruct((tok, 8), F32),
        ),
        in_specs=[pl.BlockSpec(memory_space=pltpu.SMEM), vmem, vmem, vmem],
        out_specs=(vmem, vmem, vmem),
        name="pack",
    )(c, routes, weights, tokens)


def expert_kernel(first, rows, core_ref, y_ref, x_ref, xs, *refs):
    if first:
        wg, wu, wd, out, gain_out = refs[:5]
        refs = refs[5:]
        outs = [out.at[o] for o in range(4)]
    else:
        more = refs[0:3]
        wg, wu, wd, gain_in = refs[3:7]
        outs = refs[7:11]
        refs = refs[11:]
    raw, gain_s, xn, gu_s, d_s, stage, sems, osems = refs
    core = core_ref[0]
    bit_y = jnp.bitwise_and(y_ref[0] + core, 1)
    bit_x = jnp.bitwise_and(x_ref[0] + core, 1)
    at_outer = bit_y * 2 + bit_x

    def block(o, i):
        outer = o if first else jnp.bitwise_xor(at_outer, o)
        y = jnp.bitwise_and(2 * (i >> 1) + (outer >> 1) + core, 3)
        x = jnp.bitwise_and(2 * (i & 1) + (outer & 1) + core, 3)
        return y * 4 + x

    def source(o):
        if first:
            return xs.at[o]
        return xs if o == 0 else more[o - 1]

    count = [0]

    def fetch(src, dst):
        cp = pltpu.make_async_copy(src, dst, sems.at[count[0]])
        count[0] += 1
        cp.start()
        return cp

    half = rows // 2
    width = xn.shape[1]
    units = gu_s.shape[1] // 2

    def fetch_rows(at):
        return [
            fetch(source(o).at[i, pl.ds(at, half), :], raw.at[block(o, i), pl.ds(at, half), :])
            for o in range(4)
            for i in range(4)
        ]

    x_cp = [fetch_rows(0)]
    if first:
        gain_cp = [
            fetch(source(o).at[i, pl.ds(rows, GAIN_ROWS), :], gain_s.at[block(o, i)])
            for o in range(4)
            for i in range(4)
        ]
    else:
        gain_cp = [fetch(gain_in, gain_s)]
    w_cp = [fetch(wg, gu_s.at[:, pl.ds(0, units)]), fetch(wu, gu_s.at[:, pl.ds(units, units)])]
    x_cp.append(fetch_rows(half))
    d_cp = [
        fetch(
            wd.at[:, pl.ds(pl.multiple_of(block(o, i) * 128, 128), 128)],
            d_s.at[:, pl.ds((o * 4 + i) * 128, 128)],
        )
        for o in range(4)
        for i in range(4)
    ]
    for cp in gain_cp:
        cp.wait()
    copies = []

    def store(n, src, dst):
        cp = pltpu.make_async_copy(src, dst, osems.at[n])
        cp.start()
        copies.append(cp)

    if first:
        store(4, gain_s, gain_out)
    step = 32

    def norm(i, _):
        at = pl.multiple_of(i * step, step)
        acc = jnp.zeros((step, 128), F32)
        vals = []
        for j in range(16):
            v = raw[j, pl.ds(at, step), :].astype(F32)
            vals.append(v)
            acc = acc + v * v
        scale = lax.rsqrt(jnp.sum(acc, axis=1, keepdims=True) * (1.0 / width) + EPS)
        for j in range(16):
            gain = gain_s[j, 0:1, :].astype(F32)
            xn[pl.ds(at, step), j * 128 : (j + 1) * 128] = (vals[j] * scale * gain).astype(BF16)
        return 0

    steps = half // step
    for h in range(2):
        for cp in x_cp[h]:
            cp.wait()
        lax.fori_loop(h * steps, (h + 1) * steps, norm, 0)
    for cp in w_cp:
        cp.wait()
    both = jnp.dot(xn[...], gu_s[...], preferred_element_type=F32)
    gate = both[:, :units]
    hidden = (gate * both[:, units:] / (1.0 + jnp.exp(-gate))).astype(BF16)
    for cp in d_cp:
        cp.wait()
    for o in range(4):
        res = jnp.dot(
            hidden, d_s[:, o * 512 : (o + 1) * 512], preferred_element_type=F32
        ).astype(BF16)
        for i in range(4):
            stage[o, i] = res[:, i * 128 : (i + 1) * 128]
        store(o, stage.at[o], outs[o])
    for cp in copies:
        cp.wait()


def expert(first, place, xs, weights, gain):
    rows = 512
    width, units = weights[0].shape
    hbm = pl.BlockSpec(memory_space=pltpu.HBM)
    if first:
        args = (*place, xs, *weights)
        outs = (
            jax.ShapeDtypeStruct((4, 4, rows, 128), BF16),
            jax.ShapeDtypeStruct((16, GAIN_ROWS, 128), BF16),
        )
    else:
        args = (*place, *xs, *weights, gain)
        outs = tuple([jax.ShapeDtypeStruct((4, rows, 128), BF16)] * 4)
    return pl.pallas_call(
        functools.partial(expert_kernel, first, rows),
        out_shape=outs,
        in_specs=[pl.BlockSpec(memory_space=pltpu.SMEM)] * 3 + [hbm] * (len(args) - 3),
        out_specs=tuple([hbm] * len(outs)),
        scratch_shapes=[
            pltpu.VMEM((16, rows, 128), BF16),
            pltpu.VMEM((16, GAIN_ROWS, 128), BF16),
            pltpu.VMEM((rows, width), BF16),
            pltpu.VMEM((width, 2 * units), BF16),
            pltpu.VMEM((units, width), BF16),
            pltpu.VMEM((4, 4, rows, 128), BF16),
            pltpu.SemaphoreType.DMA((66,)),
            pltpu.SemaphoreType.DMA((5,)),
        ],
        compiler_params=pltpu.CompilerParams(vmem_limit_bytes=63 * 1024 * 1024),
        name="expert_far" if first else "expert_near",
    )(*args)


def combine_kernel(table, rows, combined, squares):
    tok = table.shape[0]
    count = rows.shape[0]
    cols = lax.broadcasted_iota(jnp.int32, (tok, count), 1)
    total = None
    for k in range(2):
        target = table[:, k : k + 1].astype(jnp.int32)
        pick = (cols == target).astype(F32).astype(BF16)
        got = jnp.dot(pick, rows[...], preferred_element_type=F32)
        term = got * table[:, 2 + k : 3 + k]
        total = term if total is None else total + term
    combined[...] = total
    mine = jnp.sum((total * total).T, axis=0, keepdims=True)
    for i in range(squares.shape[0]):
        squares[i] = mine


def combine(table, rows):
    tok = table.shape[0]
    share = rows.shape[1]
    vmem = pl.BlockSpec(memory_space=pltpu.VMEM)
    return pl.pallas_call(
        combine_kernel,
        out_shape=(
            jax.ShapeDtypeStruct((tok, share), F32),
            jax.ShapeDtypeStruct((16, 1, tok), F32),
        ),
        in_specs=[vmem] * 2,
        out_specs=(vmem, vmem),
        name="combine",
    )(table, rows)


ALL = ("z", "c", "y", "x")


def flat(z, c, y, x):
    return ((z * 2 + c) * 4 + y) * 4 + x


def member(z, c, o, i):
    y = (2 * (i >> 1) + (o >> 1) + c) % 4
    x = (2 * (i & 1) + (o & 1) + c) % 4
    return flat(z, c, y, x)


PLANES = [(z, c) for z in range(16) for c in range(2)]
INNER = [[member(z, c, o, i) for i in range(4)] for z, c in PLANES for o in range(4)]
OUTER = [[member(z, c, o, i) for o in range(4)] for z, c in PLANES for i in range(4)]


def exchange(v, axis, groups=None):
    return lax.all_to_all(
        v, axis, split_axis=0, concat_axis=0, tiled=True, axis_index_groups=groups
    )


def inner_exchange(v):
    return exchange(v, ALL, INNER)


def outer_exchange(v):
    return exchange(v, ALL, OUTER)


def outer_flip(v, bits):
    pairs = [
        (member(z, c, o, i), member(z, c, o ^ bits, i))
        for z, c in PLANES
        for o in range(4)
        for i in range(4)
    ]
    return lax.ppermute(v, ALL, pairs)


def swap(v):
    return lax.ppermute(v, "c", [(0, 1), (1, 0)])


def total_of(parts):
    total = parts[0].astype(F32)
    for p in parts[1:]:
        total = total + p.astype(F32)
    return total.astype(BF16)


def summed(v):
    return total_of([v[i] for i in range(v.shape[0])])


def over_z(near, far):
    share = near.shape[1]
    both = jnp.stack([near.reshape(16, -1, share), far.reshape(16, -1, share)], axis=1)
    return exchange(both, "z")


def local(tokens, norm_gain, w_gate, w_up, w_down, routes, route_weights, final_gain):
    _, share = tokens.shape
    width = share * 16
    place = tuple(lax.axis_index(a).astype(jnp.int32).reshape(1) for a in ("c", "y", "x"))
    near, far, table = pack(place[0], routes.T, route_weights.T, tokens)
    weights = (w_gate[0], w_up[0], w_down[0])
    both = over_z(near, swap(far))
    near, far = (both[:, i].reshape(-1, share) for i in range(2))
    gain_rows = jnp.broadcast_to(norm_gain[None, :], (GAIN_ROWS, share))
    rows = jnp.concatenate([far, gain_rows, near], axis=0)
    rows = inner_exchange(jnp.broadcast_to(rows[None], (4, *rows.shape)))
    first = far.shape[0] + GAIN_ROWS
    far = rows[:, :first]
    far = outer_exchange(jnp.broadcast_to(far[None], (4, *far.shape)))
    near = rows[:, first:]
    near = [near] + [outer_flip(near, s) for s in (1, 2, 3)]
    far, gain = expert(True, place, far, weights, None)
    far = summed(outer_exchange(far))
    near = expert(False, place, near, weights, gain)
    near = total_of([near[0]] + [outer_flip(near[s], s) for s in (1, 2, 3)])
    far = swap(summed(inner_exchange(far)))
    near = summed(inner_exchange(near))
    both = over_z(near, far)
    combined, squares = combine(table, both.reshape(-1, share))
    total = exchange(squares, ("y", "x")).sum(axis=(0, 1))
    scale = lax.rsqrt(total / width + EPS)
    return (combined * scale[:, None] * final_gain.astype(F32)[None, :]).astype(BF16)


def solution(mesh):
    fine = Mesh(mesh.devices.reshape(16, 2, 4, 4), ("z", "c", "y", "x"))
    ep = ("z", "c")
    tp = ("y", "x")
    in_specs = (
        P(ep, tp),
        P(tp),
        P(ep, None, tp),
        P(ep, None, tp),
        P(ep, tp, None),
        P(ep, None),
        P(ep, None),
        P(tp),
    )
    return jax.shard_map(
        local, mesh=fine, in_specs=in_specs, out_specs=P(ep, tp), check_vma=False
    )
```

```python
import functools

import jax
import jax.numpy as jnp
from jax import lax
from jax.experimental import pallas as pl
from jax.experimental.pallas import tpu as pltpu
from jax.sharding import Mesh, PartitionSpec as P


EPS = 1e-06
F32 = jnp.float32
BF16 = jnp.bfloat16
GAIN_ROWS = 16


def pack_kernel(pos, routes, weights, tokens, out, table):
    tok = tokens.shape[0]
    count = out.shape[0]
    experts = 2 * lax.axis_size("z")
    cap = count // experts
    e0 = routes[0:1, :]
    e1 = routes[1:2, :]
    names = lax.broadcasted_iota(jnp.int32, (experts, tok), 0)
    hot0 = names == e0
    hot1 = names == e1
    hot = (hot0 | hot1).astype(F32).astype(BF16)
    row = lax.broadcasted_iota(jnp.int32, (tok, tok), 0)
    col = lax.broadcasted_iota(jnp.int32, (tok, tok), 1)
    earlier = (row < col).astype(F32).astype(BF16)
    before = jnp.dot(hot, earlier, preferred_element_type=F32)

    def place(e, mine):
        slot = jnp.sum(jnp.where(mine, before, 0.0), axis=0, keepdims=True)
        return jnp.bitwise_xor(e, pos[0]) * cap + slot.astype(jnp.int32)

    t0 = place(e0, hot0)
    t1 = place(e1, hot1)
    rows = lax.broadcasted_iota(jnp.int32, (count, tok), 0)
    put = ((rows == t0) | (rows == t1)).astype(F32).astype(BF16)
    out[...] = jnp.dot(put, tokens[...], preferred_element_type=F32).astype(BF16)
    stack = jnp.concatenate(
        [t0.astype(F32), t1.astype(F32), weights[...], jnp.zeros((4, tok), F32)], axis=0
    )
    table[...] = stack.T


def pack(c, routes, weights, tokens):
    tok, share = tokens.shape
    count = 2 * lax.axis_size("z") * 32
    vmem = pl.BlockSpec(memory_space=pltpu.VMEM)
    return pl.pallas_call(
        pack_kernel,
        out_shape=(
            jax.ShapeDtypeStruct((count, share), BF16),
            jax.ShapeDtypeStruct((tok, 8), F32),
        ),
        in_specs=[pl.BlockSpec(memory_space=pltpu.SMEM), vmem, vmem, vmem],
        out_specs=(vmem, vmem),
        name="pack",
    )(c, routes, weights, tokens)


def expert_kernel(first, rows, core_ref, y_ref, x_ref, xs, *refs):
    if first:
        wg, wu, wd, out, gain_out = refs[:5]
        refs = refs[5:]
        outs = [out.at[o] for o in range(4)]
    else:
        more = refs[0:3]
        wg, wu, wd, gain_in = refs[3:7]
        outs = refs[7:11]
        refs = refs[11:]
    raw, gain_s, xn, gu_s, d_s, stage, sems, osems = refs
    core = core_ref[0]
    role = core if first else 1 - core
    at_outer = jnp.where(role == 0, y_ref[0], x_ref[0])
    at_inner = jnp.where(role == 0, x_ref[0], y_ref[0])

    def block(o, i):
        outer = o if first else jnp.bitwise_and(at_outer + o, 3)
        return jnp.where(role == 0, outer * 4 + i, i * 4 + outer)

    def taken(o, i):
        return block(o, i if first else jnp.bitwise_and(at_inner + i, 3))

    def source(o):
        if first:
            return xs.at[o]
        return xs if o == 0 else more[o - 1]

    count = [0]

    def fetch(src, dst):
        cp = pltpu.make_async_copy(src, dst, sems.at[count[0]])
        count[0] += 1
        cp.start()
        return cp

    half = rows // 2
    width = xn.shape[1]
    units = gu_s.shape[1] // 2

    def fetch_rows(at):
        return [
            fetch(source(o).at[i, pl.ds(at, half), :], raw.at[taken(o, i), pl.ds(at, half), :])
            for o in range(4)
            for i in range(4)
        ]

    x_cp = [fetch_rows(0)]
    if first:
        gain_cp = [
            fetch(source(o).at[i, pl.ds(rows, GAIN_ROWS), :], gain_s.at[block(o, i)])
            for o in range(4)
            for i in range(4)
        ]
    else:
        gain_cp = [fetch(gain_in, gain_s)]
    w_cp = [fetch(wg, gu_s.at[:, pl.ds(0, units)]), fetch(wu, gu_s.at[:, pl.ds(units, units)])]
    x_cp.append(fetch_rows(half))
    d_cp = [
        fetch(
            wd.at[:, pl.ds(pl.multiple_of(block(o, i) * 128, 128), 128)],
            d_s.at[:, pl.ds((o * 4 + i) * 128, 128)],
        )
        for o in range(4)
        for i in range(4)
    ]
    for cp in gain_cp:
        cp.wait()
    copies = []

    def store(n, src, dst):
        cp = pltpu.make_async_copy(src, dst, osems.at[n])
        cp.start()
        copies.append(cp)

    if first:
        store(4, gain_s, gain_out)
    step = 32

    def norm(i):
        at = i * step
        acc = jnp.zeros((step, 128), F32)
        vals = []
        for j in range(16):
            v = raw[j, pl.ds(at, step), :].astype(F32)
            vals.append(v)
            acc = acc + v * v
        scale = lax.rsqrt(jnp.sum(acc, axis=1, keepdims=True) * (1.0 / width) + EPS)
        for j in range(16):
            gain = gain_s[j, 0:1, :].astype(F32)
            xn[pl.ds(at, step), j * 128 : (j + 1) * 128] = (vals[j] * scale * gain).astype(BF16)

    steps = half // step

    def act(gate, up):
        return (gate * up / (1.0 + jnp.exp(-gate))).astype(BF16)

    for cp in x_cp[0]:
        cp.wait()
    for i in range(steps):
        norm(i)
    w_cp[0].wait()
    gate = jnp.dot(xn[:half, :], gu_s[:, :units], preferred_element_type=F32)
    w_cp[1].wait()
    for cp in x_cp[1]:
        cp.wait()
    up = jnp.dot(xn[:half, :], gu_s[:, units:], preferred_element_type=F32)
    low = act(gate, up)
    for i in range(steps, 2 * steps):
        norm(i)
    both = jnp.dot(xn[half:, :], gu_s[...], preferred_element_type=F32)
    hidden = jnp.concatenate([low, act(both[:, :units], both[:, units:])], axis=0)
    for cp in d_cp:
        cp.wait()
    for o in range(4):
        res = jnp.dot(
            hidden, d_s[:, o * 512 : (o + 1) * 512], preferred_element_type=F32
        ).astype(BF16)
        for i in range(4):
            stage[o, i] = res[:, i * 128 : (i + 1) * 128]
        store(o, stage.at[o], outs[o])
    for cp in copies:
        cp.wait()


def expert(first, place, xs, weights, gain):
    rows = 512
    width, units = weights[0].shape
    hbm = pl.BlockSpec(memory_space=pltpu.HBM)
    if first:
        args = (*place, xs, *weights)
        outs = (
            jax.ShapeDtypeStruct((4, 4, rows, 128), BF16),
            jax.ShapeDtypeStruct((16, GAIN_ROWS, 128), BF16),
        )
    else:
        args = (*place, *xs, *weights, gain)
        outs = tuple([jax.ShapeDtypeStruct((4, rows, 128), BF16)] * 4)
    return pl.pallas_call(
        functools.partial(expert_kernel, first, rows),
        out_shape=outs,
        in_specs=[pl.BlockSpec(memory_space=pltpu.SMEM)] * 3 + [hbm] * (len(args) - 3),
        out_specs=tuple([hbm] * len(outs)),
        scratch_shapes=[
            pltpu.VMEM((16, rows, 128), BF16),
            pltpu.VMEM((16, GAIN_ROWS, 128), BF16),
            pltpu.VMEM((rows, width), BF16),
            pltpu.VMEM((width, 2 * units), BF16),
            pltpu.VMEM((units, width), BF16),
            pltpu.VMEM((4, 4, rows, 128), BF16),
            pltpu.SemaphoreType.DMA((66,)),
            pltpu.SemaphoreType.DMA((5,)),
        ],
        compiler_params=pltpu.CompilerParams(vmem_limit_bytes=63 * 1024 * 1024),
        name="expert_far" if first else "expert_near",
    )(*args)


def combine_kernel(table, rows, combined, squares):
    tok = table.shape[0]
    count = rows.shape[0]
    cols = lax.broadcasted_iota(jnp.int32, (tok, count), 1)
    total = None
    for k in range(2):
        target = table[:, k : k + 1].astype(jnp.int32)
        pick = (cols == target).astype(F32).astype(BF16)
        got = jnp.dot(pick, rows[...], preferred_element_type=F32)
        term = got * table[:, 2 + k : 3 + k]
        total = term if total is None else total + term
    combined[...] = total
    mine = jnp.sum((total * total).T, axis=0, keepdims=True)
    for i in range(squares.shape[0]):
        squares[i] = mine


def combine(table, rows):
    tok = table.shape[0]
    share = rows.shape[1]
    vmem = pl.BlockSpec(memory_space=pltpu.VMEM)
    return pl.pallas_call(
        combine_kernel,
        out_shape=(
            jax.ShapeDtypeStruct((tok, share), F32),
            jax.ShapeDtypeStruct((16, 1, tok), F32),
        ),
        in_specs=[vmem] * 2,
        out_specs=(vmem, vmem),
        name="combine",
    )(table, rows)


ALL = ("z", "c", "y", "x")


def flat(z, c, y, x):
    return ((z * 2 + c) * 4 + y) * 4 + x


def lines(along_x_for):
    groups = []
    for z in range(16):
        for c in range(2):
            for i in range(4):
                if c == along_x_for:
                    groups.append([flat(z, c, i, x) for x in range(4)])
                else:
                    groups.append([flat(z, c, y, i) for y in range(4)])
    return groups


def exchange(v, axis, groups=None):
    return lax.all_to_all(
        v, axis, split_axis=0, concat_axis=0, tiled=True, axis_index_groups=groups
    )


def across(v, along_x_for):
    return exchange(v, ALL, lines(along_x_for))


def ahead(v, along_x_for, step):
    pairs = []
    for z in range(16):
        for c in range(2):
            for y in range(4):
                for x in range(4):
                    to_y, to_x = (y, x + step) if c == along_x_for else (y + step, x)
                    pairs.append((flat(z, c, y, x), flat(z, c, to_y % 4, to_x % 4)))
    return lax.ppermute(v, ALL, pairs)


def swap(v):
    return lax.ppermute(v, "c", [(0, 1), (1, 0)])


def total_of(parts):
    total = parts[0].astype(F32)
    for p in parts[1:]:
        total = total + p.astype(F32)
    return total.astype(BF16)


def summed(v):
    return total_of([v[i] for i in range(v.shape[0])])


def copies_of(v):
    return jnp.broadcast_to(v[None], (4, *v.shape))


def local(tokens, norm_gain, w_gate, w_up, w_down, routes, route_weights, final_gain):
    _, share = tokens.shape
    width = share * 16
    place = tuple(lax.axis_index(a).astype(jnp.int32).reshape(1) for a in ("c", "y", "x"))
    rows, table = pack(place[0], routes.T, route_weights.T, tokens)
    weights = (w_gate[0], w_up[0], w_down[0])
    both = exchange(rows.reshape(16, 2, -1, share), "z")
    near, far = (both[:, i].reshape(-1, share) for i in range(2))
    far = swap(far)
    gain_rows = jnp.broadcast_to(norm_gain[None, :], (GAIN_ROWS, share))
    far = across(copies_of(jnp.concatenate([far, gain_rows], axis=0)), 0)
    near = jnp.stack([near] + [ahead(near, 1, -s) for s in (1, 2, 3)])
    far = across(copies_of(far), 1)
    near = [near] + [ahead(near, 0, -s) for s in (1, 2, 3)]
    far, gain = expert(True, place, far, weights, None)
    far = summed(across(far, 1))
    near = expert(False, place, near, weights, gain)
    two = ahead(near[2], 0, 2)
    near = total_of([near[0], two, ahead(near[1], 0, 1), ahead(near[3], 0, 3)])
    far = swap(summed(across(far, 0)))
    near = summed(across(near, 1))
    both = jnp.stack([near.reshape(16, -1, share), far.reshape(16, -1, share)], axis=1)
    combined, squares = combine(table, exchange(both, "z").reshape(-1, share))
    total = exchange(squares, ("y", "x")).sum(axis=(0, 1))
    scale = lax.rsqrt(total / width + EPS)
    return (combined * scale[:, None] * final_gain.astype(F32)[None, :]).astype(BF16)


def solution(mesh):
    fine = Mesh(mesh.devices.reshape(16, 2, 4, 4), ("z", "c", "y", "x"))
    ep = ("z", "c")
    tp = ("y", "x")
    in_specs = (
        P(ep, tp),
        P(tp),
        P(ep, None, tp),
        P(ep, None, tp),
        P(ep, tp, None),
        P(ep, None),
        P(ep, None),
        P(tp),
    )
    return jax.shard_map(
        local, mesh=fine, in_specs=in_specs, out_specs=P(ep, tp), check_vma=False
    )
```

```python
import functools

import jax
import jax.numpy as jnp
from jax import lax
from jax.experimental import pallas as pl
from jax.experimental.pallas import tpu as pltpu
from jax.sharding import Mesh, PartitionSpec as P


EPS = 1e-06
F32 = jnp.float32
BF16 = jnp.bfloat16
GAIN_ROWS = 16


def pack_kernel(pos, routes, weights, tokens, near, far, table):
    tok = tokens.shape[0]
    half = near.shape[0]
    experts = 2 * lax.axis_size("z")
    cap = half // (experts // 2)
    e0 = routes[0:1, :]
    e1 = routes[1:2, :]
    lanes = lax.broadcasted_iota(jnp.int32, (experts, tok), 0)
    hot0 = lanes == e0
    hot1 = lanes == e1
    hot = (hot0 | hot1).astype(F32).astype(BF16)
    row = lax.broadcasted_iota(jnp.int32, (tok, tok), 0)
    col = lax.broadcasted_iota(jnp.int32, (tok, tok), 1)
    earlier = (row < col).astype(F32).astype(BF16)
    before = jnp.dot(hot, earlier, preferred_element_type=F32)

    def place(e, mine):
        slot = jnp.sum(jnp.where(mine, before, 0.0), axis=0, keepdims=True)
        other = jnp.bitwise_xor(jnp.bitwise_and(e, 1), pos[0])
        return other * half + (e >> 1) * cap + slot.astype(jnp.int32)

    t0 = place(e0, hot0)
    t1 = place(e1, hot1)
    for at, out in ((0, near), (half, far)):
        rows = lax.broadcasted_iota(jnp.int32, (half, tok), 0) + at
        put = ((rows == t0) | (rows == t1)).astype(F32).astype(BF16)
        out[...] = jnp.dot(put, tokens[...], preferred_element_type=F32).astype(BF16)

    def packed(t):
        other = (t >= half).astype(jnp.int32)
        inside = t - other * half
        at_z = inside // cap
        return (at_z * 2 + other) * cap + (inside - at_z * cap)

    t0 = packed(t0)
    t1 = packed(t1)
    stack = jnp.concatenate(
        [t0.astype(F32), t1.astype(F32), weights[...], jnp.zeros((4, tok), F32)], axis=0
    )
    table[...] = stack.T


def pack(c, routes, weights, tokens):
    tok, share = tokens.shape
    half = lax.axis_size("z") * 32
    vmem = pl.BlockSpec(memory_space=pltpu.VMEM)
    return pl.pallas_call(
        pack_kernel,
        out_shape=(
            jax.ShapeDtypeStruct((half, share), BF16),
            jax.ShapeDtypeStruct((half, share), BF16),
            jax.ShapeDtypeStruct((tok, 8), F32),
        ),
        in_specs=[pl.BlockSpec(memory_space=pltpu.SMEM), vmem, vmem, vmem],
        out_specs=(vmem, vmem, vmem),
        name="pack",
    )(c, routes, weights, tokens)


def expert_kernel(first, rows, core_ref, y_ref, x_ref, xs, *refs):
    if first:
        wg, wu, wd, out, gain_out = refs[:5]
        refs = refs[5:]
        outs = [out.at[o] for o in range(4)]
    else:
        more = refs[0:3]
        wg, wu, wd, gain_in = refs[3:7]
        outs = refs[7:11]
        refs = refs[11:]
    raw, gain_s, xn, gu_s, d_s, stage, sems, osems = refs
    core = core_ref[0]
    at_outer = jnp.where(core == 0, y_ref[0], x_ref[0])

    def block(o, i):
        outer = o if first else jnp.bitwise_and(at_outer + o, 3)
        return jnp.where(core == 0, outer * 4 + i, i * 4 + outer)

    def sent(o, i):
        if first:
            return block(o, i)
        outer = jnp.bitwise_and(jnp.where(core == 0, x_ref[0], y_ref[0]) + o, 3)
        return jnp.where(core == 0, i * 4 + outer, outer * 4 + i)

    def source(o):
        if first:
            return xs.at[o]
        return xs if o == 0 else more[o - 1]

    count = [0]

    def fetch(src, dst):
        cp = pltpu.make_async_copy(src, dst, sems.at[count[0]])
        count[0] += 1
        cp.start()
        return cp

    half = rows // 2
    width = xn.shape[1]
    units = gu_s.shape[1] // 2

    def fetch_rows(at):
        return [
            fetch(source(o).at[i, pl.ds(at, half), :], raw.at[block(o, i), pl.ds(at, half), :])
            for o in range(4)
            for i in range(4)
        ]

    x_cp = [fetch_rows(0)]
    if first:
        gain_cp = [
            fetch(source(o).at[i, pl.ds(rows, GAIN_ROWS), :], gain_s.at[block(o, i)])
            for o in range(4)
            for i in range(4)
        ]
    else:
        gain_cp = [fetch(gain_in, gain_s)]
    w_cp = [fetch(wg, gu_s.at[:, pl.ds(0, units)]), fetch(wu, gu_s.at[:, pl.ds(units, units)])]
    x_cp.append(fetch_rows(half))
    d_cp = [
        fetch(
            wd.at[:, pl.ds(pl.multiple_of(sent(o, i) * 128, 128), 128)],
            d_s.at[:, pl.ds((o * 4 + i) * 128, 128)],
        )
        for o in range(4)
        for i in range(4)
    ]
    for cp in gain_cp:
        cp.wait()
    copies = []

    def store(n, src, dst):
        cp = pltpu.make_async_copy(src, dst, osems.at[n])
        cp.start()
        copies.append(cp)

    if first:
        store(4, gain_s, gain_out)
    step = 32

    def norm(i):
        at = i * step
        acc = jnp.zeros((step, 128), F32)
        vals = []
        for j in range(16):
            v = raw[j, pl.ds(at, step), :].astype(F32)
            vals.append(v)
            acc = acc + v * v
        scale = lax.rsqrt(jnp.sum(acc, axis=1, keepdims=True) * (1.0 / width) + EPS)
        for j in range(16):
            gain = gain_s[j, 0:1, :].astype(F32)
            xn[pl.ds(at, step), j * 128 : (j + 1) * 128] = (vals[j] * scale * gain).astype(BF16)

    steps = half // step

    def act(gate, up):
        return (gate * up / (1.0 + jnp.exp(-gate))).astype(BF16)

    for cp in x_cp[0]:
        cp.wait()
    for i in range(steps):
        norm(i)
    w_cp[0].wait()
    gate = jnp.dot(xn[:half, :], gu_s[:, :units], preferred_element_type=F32)
    w_cp[1].wait()
    for cp in x_cp[1]:
        cp.wait()
    up = jnp.dot(xn[:half, :], gu_s[:, units:], preferred_element_type=F32)
    low = act(gate, up)
    for i in range(steps, 2 * steps):
        norm(i)
    both = jnp.dot(xn[half:, :], gu_s[...], preferred_element_type=F32)
    hidden = jnp.concatenate([low, act(both[:, :units], both[:, units:])], axis=0)
    for cp in d_cp:
        cp.wait()
    for o in range(4):
        res = jnp.dot(
            hidden, d_s[:, o * 512 : (o + 1) * 512], preferred_element_type=F32
        ).astype(BF16)
        for i in range(4):
            stage[o, i] = res[:, i * 128 : (i + 1) * 128]
        store(o, stage.at[o], outs[o])
    for cp in copies:
        cp.wait()


def expert(first, place, xs, weights, gain):
    rows = 512
    width, units = weights[0].shape
    hbm = pl.BlockSpec(memory_space=pltpu.HBM)
    if first:
        args = (*place, xs, *weights)
        outs = (
            jax.ShapeDtypeStruct((4, 4, rows, 128), BF16),
            jax.ShapeDtypeStruct((16, GAIN_ROWS, 128), BF16),
        )
    else:
        args = (*place, *xs, *weights, gain)
        outs = tuple([jax.ShapeDtypeStruct((4, rows, 128), BF16)] * 4)
    return pl.pallas_call(
        functools.partial(expert_kernel, first, rows),
        out_shape=outs,
        in_specs=[pl.BlockSpec(memory_space=pltpu.SMEM)] * 3 + [hbm] * (len(args) - 3),
        out_specs=tuple([hbm] * len(outs)),
        scratch_shapes=[
            pltpu.VMEM((16, rows, 128), BF16),
            pltpu.VMEM((16, GAIN_ROWS, 128), BF16),
            pltpu.VMEM((rows, width), BF16),
            pltpu.VMEM((width, 2 * units), BF16),
            pltpu.VMEM((units, width), BF16),
            pltpu.VMEM((4, 4, rows, 128), BF16),
            pltpu.SemaphoreType.DMA((66,)),
            pltpu.SemaphoreType.DMA((5,)),
        ],
        compiler_params=pltpu.CompilerParams(vmem_limit_bytes=63 * 1024 * 1024),
        name="expert_far" if first else "expert_near",
    )(*args)


def combine_kernel(table, rows, combined, squares):
    tok = table.shape[0]
    count = rows.shape[0]
    cols = lax.broadcasted_iota(jnp.int32, (tok, count), 1)
    total = None
    for k in range(2):
        target = table[:, k : k + 1].astype(jnp.int32)
        pick = (cols == target).astype(F32).astype(BF16)
        got = jnp.dot(pick, rows[...], preferred_element_type=F32)
        term = got * table[:, 2 + k : 3 + k]
        total = term if total is None else total + term
    combined[...] = total
    mine = jnp.sum((total * total).T, axis=0, keepdims=True)
    for i in range(squares.shape[0]):
        squares[i] = mine


def combine(table, rows):
    tok = table.shape[0]
    share = rows.shape[1]
    vmem = pl.BlockSpec(memory_space=pltpu.VMEM)
    return pl.pallas_call(
        combine_kernel,
        out_shape=(
            jax.ShapeDtypeStruct((tok, share), F32),
            jax.ShapeDtypeStruct((16, 1, tok), F32),
        ),
        in_specs=[vmem] * 2,
        out_specs=(vmem, vmem),
        name="combine",
    )(table, rows)


ALL = ("z", "c", "y", "x")


def flat(z, c, y, x):
    return ((z * 2 + c) * 4 + y) * 4 + x


def lines(along_x_for):
    groups = []
    for z in range(16):
        for c in range(2):
            for i in range(4):
                if c == along_x_for:
                    groups.append([flat(z, c, i, x) for x in range(4)])
                else:
                    groups.append([flat(z, c, y, i) for y in range(4)])
    return groups


def exchange(v, axis, groups=None):
    return lax.all_to_all(
        v, axis, split_axis=0, concat_axis=0, tiled=True, axis_index_groups=groups
    )


def across(v, along_x_for):
    return exchange(v, ALL, lines(along_x_for))


def ahead(v, along_x_for, step):
    pairs = []
    for z in range(16):
        for c in range(2):
            for y in range(4):
                for x in range(4):
                    to_y, to_x = (y, x + step) if c == along_x_for else (y + step, x)
                    pairs.append((flat(z, c, y, x), flat(z, c, to_y % 4, to_x % 4)))
    return lax.ppermute(v, ALL, pairs)


def swap(v):
    return lax.ppermute(v, "c", [(0, 1), (1, 0)])


def total_of(parts):
    total = parts[0].astype(F32)
    for p in parts[1:]:
        total = total + p.astype(F32)
    return total.astype(BF16)


def summed(v):
    return total_of([v[i] for i in range(v.shape[0])])


def copies_of(v):
    return jnp.broadcast_to(v[None], (4, *v.shape))


def over_z(near, far):
    share = near.shape[1]
    both = jnp.stack([near.reshape(16, -1, share), far.reshape(16, -1, share)], axis=1)
    return exchange(both, "z")


def local(tokens, norm_gain, w_gate, w_up, w_down, routes, route_weights, final_gain):
    _, share = tokens.shape
    width = share * 16
    place = tuple(lax.axis_index(a).astype(jnp.int32).reshape(1) for a in ("c", "y", "x"))
    near, far, table = pack(place[0], routes.T, route_weights.T, tokens)
    weights = (w_gate[0], w_up[0], w_down[0])
    both = over_z(near, swap(far))
    near, far = (both[:, i].reshape(-1, share) for i in range(2))
    gain_rows = jnp.broadcast_to(norm_gain[None, :], (GAIN_ROWS, share))
    rows = jnp.concatenate([far, gain_rows, near], axis=0)
    rows = across(copies_of(rows), 0)
    first = far.shape[0] + GAIN_ROWS
    far = across(copies_of(rows[:, :first]), 1)
    near = rows[:, first:]
    near = [near] + [ahead(near, 1, -s) for s in (1, 2, 3)]
    far, gain = expert(True, place, far, weights, None)
    far = summed(across(far, 1))
    near = expert(False, place, near, weights, gain)
    two = ahead(near[2], 0, 2)
    near = total_of([near[0], two, ahead(near[1], 0, 1), ahead(near[3], 0, 3)])
    far = swap(summed(across(far, 0)))
    near = summed(across(near, 1))
    both = over_z(near, far)
    combined, squares = combine(table, both.reshape(-1, share))
    total = exchange(squares, ("y", "x")).sum(axis=(0, 1))
    scale = lax.rsqrt(total / width + EPS)
    return (combined * scale[:, None] * final_gain.astype(F32)[None, :]).astype(BF16)


def solution(mesh):
    fine = Mesh(mesh.devices.reshape(16, 2, 4, 4), ("z", "c", "y", "x"))
    ep = ("z", "c")
    tp = ("y", "x")
    in_specs = (
        P(ep, tp),
        P(tp),
        P(ep, None, tp),
        P(ep, None, tp),
        P(ep, tp, None),
        P(ep, None),
        P(ep, None),
        P(tp),
    )
    return jax.shard_map(
        local, mesh=fine, in_specs=in_specs, out_specs=P(ep, tp), check_vma=False
    )
```

```python
import functools

import jax
import jax.numpy as jnp
from jax import lax
from jax.experimental import pallas as pl
from jax.experimental.pallas import tpu as pltpu
from jax.sharding import Mesh, PartitionSpec as P


EPS = 1e-06
F32 = jnp.float32
BF16 = jnp.bfloat16
GAIN_ROWS = 16


def pack_kernel(pos, routes, weights, tokens, near, far, table):
    tok = tokens.shape[0]
    half = near.shape[0]
    experts = 2 * lax.axis_size("z")
    cap = half // (experts // 2)
    e0 = routes[0:1, :]
    e1 = routes[1:2, :]
    lanes = lax.broadcasted_iota(jnp.int32, (experts, tok), 0)
    hot0 = lanes == e0
    hot1 = lanes == e1
    hot = (hot0 | hot1).astype(F32).astype(BF16)
    row = lax.broadcasted_iota(jnp.int32, (tok, tok), 0)
    col = lax.broadcasted_iota(jnp.int32, (tok, tok), 1)
    earlier = (row < col).astype(F32).astype(BF16)
    before = jnp.dot(hot, earlier, preferred_element_type=F32)

    def place(e, mine):
        slot = jnp.sum(jnp.where(mine, before, 0.0), axis=0, keepdims=True)
        other = jnp.bitwise_xor(jnp.bitwise_and(e, 1), pos[0])
        return other * half + (e >> 1) * cap + slot.astype(jnp.int32)

    t0 = place(e0, hot0)
    t1 = place(e1, hot1)
    for at, out in ((0, near), (half, far)):
        rows = lax.broadcasted_iota(jnp.int32, (half, tok), 0) + at
        put = ((rows == t0) | (rows == t1)).astype(F32).astype(BF16)
        out[...] = jnp.dot(put, tokens[...], preferred_element_type=F32).astype(BF16)

    def packed(t):
        other = (t >= half).astype(jnp.int32)
        inside = t - other * half
        at_z = inside // cap
        return (at_z * 2 + other) * cap + (inside - at_z * cap)

    t0 = packed(t0)
    t1 = packed(t1)
    stack = jnp.concatenate(
        [t0.astype(F32), t1.astype(F32), weights[...], jnp.zeros((4, tok), F32)], axis=0
    )
    table[...] = stack.T


def pack(c, routes, weights, tokens):
    tok, share = tokens.shape
    half = lax.axis_size("z") * 32
    vmem = pl.BlockSpec(memory_space=pltpu.VMEM)
    return pl.pallas_call(
        pack_kernel,
        out_shape=(
            jax.ShapeDtypeStruct((half, share), BF16),
            jax.ShapeDtypeStruct((half, share), BF16),
            jax.ShapeDtypeStruct((tok, 8), F32),
        ),
        in_specs=[pl.BlockSpec(memory_space=pltpu.SMEM), vmem, vmem, vmem],
        out_specs=(vmem, vmem, vmem),
        name="pack",
    )(c, routes, weights, tokens)


def expert_kernel(first, rows, core_ref, y_ref, x_ref, xs, *refs):
    if first:
        wg, wu, wd, out, gain_out = refs[:5]
        refs = refs[5:]
        outs = [out.at[o] for o in range(4)]
    else:
        more = refs[0:3]
        wg, wu, wd, gain_in = refs[3:7]
        outs = refs[7:11]
        refs = refs[11:]
    raw, gain_s, xn, gu_s, d_s, stage, sems, osems = refs
    core = core_ref[0]
    at_outer = jnp.where(core == 0, y_ref[0], x_ref[0])

    def block(o, i):
        outer = o if first else jnp.bitwise_and(at_outer + o, 3)
        return jnp.where(core == 0, outer * 4 + i, i * 4 + outer)

    def sent(o, i):
        if first:
            return block(o, i)
        y = jnp.bitwise_and(y_ref[0] + jnp.where(core == 0, i, o), 3)
        x = jnp.bitwise_and(x_ref[0] + jnp.where(core == 0, o, i), 3)
        return y * 4 + x

    def source(o):
        if first:
            return xs.at[o]
        return xs if o == 0 else more[o - 1]

    count = [0]

    def fetch(src, dst):
        cp = pltpu.make_async_copy(src, dst, sems.at[count[0]])
        count[0] += 1
        cp.start()
        return cp

    half = rows // 2
    width = xn.shape[1]
    units = gu_s.shape[1] // 2

    def fetch_rows(at):
        return [
            fetch(source(o).at[i, pl.ds(at, half), :], raw.at[block(o, i), pl.ds(at, half), :])
            for o in range(4)
            for i in range(4)
        ]

    x_cp = [fetch_rows(0)]
    if first:
        gain_cp = [
            fetch(source(o).at[i, pl.ds(rows, GAIN_ROWS), :], gain_s.at[block(o, i)])
            for o in range(4)
            for i in range(4)
        ]
    else:
        gain_cp = [fetch(gain_in, gain_s)]
    w_cp = [fetch(wg, gu_s.at[:, pl.ds(0, units)]), fetch(wu, gu_s.at[:, pl.ds(units, units)])]
    x_cp.append(fetch_rows(half))
    d_cp = [
        fetch(
            wd.at[:, pl.ds(pl.multiple_of(sent(o, i) * 128, 128), 128)],
            d_s.at[:, pl.ds((o * 4 + i) * 128, 128)],
        )
        for o in range(4)
        for i in range(4)
    ]
    for cp in gain_cp:
        cp.wait()
    copies = []

    def store(n, src, dst):
        cp = pltpu.make_async_copy(src, dst, osems.at[n])
        cp.start()
        copies.append(cp)

    if first:
        store(4, gain_s, gain_out)
    step = 32

    def norm(i):
        at = i * step
        acc = jnp.zeros((step, 128), F32)
        vals = []
        for j in range(16):
            v = raw[j, pl.ds(at, step), :].astype(F32)
            vals.append(v)
            acc = acc + v * v
        scale = lax.rsqrt(jnp.sum(acc, axis=1, keepdims=True) * (1.0 / width) + EPS)
        for j in range(16):
            gain = gain_s[j, 0:1, :].astype(F32)
            xn[pl.ds(at, step), j * 128 : (j + 1) * 128] = (vals[j] * scale * gain).astype(BF16)

    steps = half // step

    def act(gate, up):
        return (gate * up / (1.0 + jnp.exp(-gate))).astype(BF16)

    for cp in x_cp[0]:
        cp.wait()
    for i in range(steps):
        norm(i)
    w_cp[0].wait()
    gate = jnp.dot(xn[:half, :], gu_s[:, :units], preferred_element_type=F32)
    w_cp[1].wait()
    for cp in x_cp[1]:
        cp.wait()
    up = jnp.dot(xn[:half, :], gu_s[:, units:], preferred_element_type=F32)
    low = act(gate, up)
    for i in range(steps, 2 * steps):
        norm(i)
    both = jnp.dot(xn[half:, :], gu_s[...], preferred_element_type=F32)
    hidden = jnp.concatenate([low, act(both[:, :units], both[:, units:])], axis=0)
    for cp in d_cp:
        cp.wait()
    for o in range(4):
        res = jnp.dot(
            hidden, d_s[:, o * 512 : (o + 1) * 512], preferred_element_type=F32
        ).astype(BF16)
        for i in range(4):
            stage[o, i] = res[:, i * 128 : (i + 1) * 128]
        store(o, stage.at[o], outs[o])
    for cp in copies:
        cp.wait()


def expert(first, place, xs, weights, gain):
    rows = 512
    width, units = weights[0].shape
    hbm = pl.BlockSpec(memory_space=pltpu.HBM)
    if first:
        args = (*place, xs, *weights)
        outs = (
            jax.ShapeDtypeStruct((4, 4, rows, 128), BF16),
            jax.ShapeDtypeStruct((16, GAIN_ROWS, 128), BF16),
        )
    else:
        args = (*place, *xs, *weights, gain)
        outs = tuple([jax.ShapeDtypeStruct((4, rows, 128), BF16)] * 4)
    return pl.pallas_call(
        functools.partial(expert_kernel, first, rows),
        out_shape=outs,
        in_specs=[pl.BlockSpec(memory_space=pltpu.SMEM)] * 3 + [hbm] * (len(args) - 3),
        out_specs=tuple([hbm] * len(outs)),
        scratch_shapes=[
            pltpu.VMEM((16, rows, 128), BF16),
            pltpu.VMEM((16, GAIN_ROWS, 128), BF16),
            pltpu.VMEM((rows, width), BF16),
            pltpu.VMEM((width, 2 * units), BF16),
            pltpu.VMEM((units, width), BF16),
            pltpu.VMEM((4, 4, rows, 128), BF16),
            pltpu.SemaphoreType.DMA((66,)),
            pltpu.SemaphoreType.DMA((5,)),
        ],
        compiler_params=pltpu.CompilerParams(vmem_limit_bytes=63 * 1024 * 1024),
        name="expert_far" if first else "expert_near",
    )(*args)


def combine_kernel(table, rows, combined, squares):
    tok = table.shape[0]
    count = rows.shape[0]
    cols = lax.broadcasted_iota(jnp.int32, (tok, count), 1)
    total = None
    for k in range(2):
        target = table[:, k : k + 1].astype(jnp.int32)
        pick = (cols == target).astype(F32).astype(BF16)
        got = jnp.dot(pick, rows[...], preferred_element_type=F32)
        term = got * table[:, 2 + k : 3 + k]
        total = term if total is None else total + term
    combined[...] = total
    mine = jnp.sum((total * total).T, axis=0, keepdims=True)
    for i in range(squares.shape[0]):
        squares[i] = mine


def combine(table, rows):
    tok = table.shape[0]
    share = rows.shape[1]
    vmem = pl.BlockSpec(memory_space=pltpu.VMEM)
    return pl.pallas_call(
        combine_kernel,
        out_shape=(
            jax.ShapeDtypeStruct((tok, share), F32),
            jax.ShapeDtypeStruct((16, 1, tok), F32),
        ),
        in_specs=[vmem] * 2,
        out_specs=(vmem, vmem),
        name="combine",
    )(table, rows)


ALL = ("z", "c", "y", "x")


def flat(z, c, y, x):
    return ((z * 2 + c) * 4 + y) * 4 + x


def lines(along_x_for):
    groups = []
    for z in range(16):
        for c in range(2):
            for i in range(4):
                if c == along_x_for:
                    groups.append([flat(z, c, i, x) for x in range(4)])
                else:
                    groups.append([flat(z, c, y, i) for y in range(4)])
    return groups


def exchange(v, axis, groups=None):
    return lax.all_to_all(
        v, axis, split_axis=0, concat_axis=0, tiled=True, axis_index_groups=groups
    )


def across(v, along_x_for):
    return exchange(v, ALL, lines(along_x_for))


def ahead(v, along_x_for, step):
    pairs = []
    for z in range(16):
        for c in range(2):
            for y in range(4):
                for x in range(4):
                    to_y, to_x = (y, x + step) if c == along_x_for else (y + step, x)
                    pairs.append((flat(z, c, y, x), flat(z, c, to_y % 4, to_x % 4)))
    return lax.ppermute(v, ALL, pairs)


def swap(v):
    return lax.ppermute(v, "c", [(0, 1), (1, 0)])


def total_of(parts):
    total = parts[0].astype(F32)
    for p in parts[1:]:
        total = total + p.astype(F32)
    return total.astype(BF16)


def summed(v):
    return total_of([v[i] for i in range(v.shape[0])])


def copies_of(v):
    return jnp.broadcast_to(v[None], (4, *v.shape))


def over_z(near, far):
    share = near.shape[1]
    both = jnp.stack([near.reshape(16, -1, share), far.reshape(16, -1, share)], axis=1)
    return exchange(both, "z")


def local(tokens, norm_gain, w_gate, w_up, w_down, routes, route_weights, final_gain):
    _, share = tokens.shape
    width = share * 16
    place = tuple(lax.axis_index(a).astype(jnp.int32).reshape(1) for a in ("c", "y", "x"))
    near, far, table = pack(place[0], routes.T, route_weights.T, tokens)
    weights = (w_gate[0], w_up[0], w_down[0])
    both = over_z(near, swap(far))
    near, far = (both[:, i].reshape(-1, share) for i in range(2))
    gain_rows = jnp.broadcast_to(norm_gain[None, :], (GAIN_ROWS, share))
    rows = jnp.concatenate([far, gain_rows, near], axis=0)
    rows = across(copies_of(rows), 0)
    first = far.shape[0] + GAIN_ROWS
    far = across(copies_of(rows[:, :first]), 1)
    near = rows[:, first:]
    near = [near] + [ahead(near, 1, -s) for s in (1, 2, 3)]
    far, gain = expert(True, place, far, weights, None)
    far = summed(across(far, 1))
    near = expert(False, place, near, weights, gain)
    two = ahead(near[2], 0, 2)
    near = (near[0], two, ahead(near[1], 0, 1), ahead(near[3], 0, 3))
    near = [total_of([v[i] for v in near]) for i in range(4)]
    far = swap(summed(across(far, 0)))
    near = total_of([near[0]] + [ahead(near[s], 1, s) for s in (1, 2, 3)])
    both = over_z(near, far)
    combined, squares = combine(table, both.reshape(-1, share))
    total = exchange(squares, ("y", "x")).sum(axis=(0, 1))
    scale = lax.rsqrt(total / width + EPS)
    return (combined * scale[:, None] * final_gain.astype(F32)[None, :]).astype(BF16)


def solution(mesh):
    fine = Mesh(mesh.devices.reshape(16, 2, 4, 4), ("z", "c", "y", "x"))
    ep = ("z", "c")
    tp = ("y", "x")
    in_specs = (
        P(ep, tp),
        P(tp),
        P(ep, None, tp),
        P(ep, None, tp),
        P(ep, tp, None),
        P(ep, None),
        P(ep, None),
        P(tp),
    )
    return jax.shard_map(
        local, mesh=fine, in_specs=in_specs, out_specs=P(ep, tp), check_vma=False
    )
```

```python
import functools

import jax
import jax.numpy as jnp
from jax import lax
from jax.experimental import pallas as pl
from jax.experimental.pallas import tpu as pltpu
from jax.sharding import Mesh, PartitionSpec as P


EPS = 1e-06
F32 = jnp.float32
BF16 = jnp.bfloat16
GAIN_ROWS = 16


def pack_kernel(pos, routes, weights, tokens, near, far, table):
    tok = tokens.shape[0]
    half = near.shape[0]
    experts = 2 * lax.axis_size("z")
    cap = half // (experts // 2)
    e0 = routes[0:1, :]
    e1 = routes[1:2, :]
    lanes = lax.broadcasted_iota(jnp.int32, (experts, tok), 0)
    hot0 = lanes == e0
    hot1 = lanes == e1
    hot = (hot0 | hot1).astype(F32).astype(BF16)
    row = lax.broadcasted_iota(jnp.int32, (tok, tok), 0)
    col = lax.broadcasted_iota(jnp.int32, (tok, tok), 1)
    earlier = (row < col).astype(F32).astype(BF16)
    before = jnp.dot(hot, earlier, preferred_element_type=F32)

    def place(e, mine):
        slot = jnp.sum(jnp.where(mine, before, 0.0), axis=0, keepdims=True)
        other = jnp.bitwise_xor(jnp.bitwise_and(e, 1), pos[0])
        return other * half + (e >> 1) * cap + slot.astype(jnp.int32)

    t0 = place(e0, hot0)
    t1 = place(e1, hot1)
    for at, out in ((0, near), (half, far)):
        rows = lax.broadcasted_iota(jnp.int32, (half, tok), 0) + at
        put = ((rows == t0) | (rows == t1)).astype(F32).astype(BF16)
        out[...] = jnp.dot(put, tokens[...], preferred_element_type=F32).astype(BF16)

    def packed(t):
        other = (t >= half).astype(jnp.int32)
        inside = t - other * half
        at_z = inside // cap
        return (at_z * 2 + other) * cap + (inside - at_z * cap)

    t0 = packed(t0)
    t1 = packed(t1)
    stack = jnp.concatenate(
        [t0.astype(F32), t1.astype(F32), weights[...], jnp.zeros((4, tok), F32)], axis=0
    )
    table[...] = stack.T


def pack(c, routes, weights, tokens):
    tok, share = tokens.shape
    half = lax.axis_size("z") * 32
    vmem = pl.BlockSpec(memory_space=pltpu.VMEM)
    return pl.pallas_call(
        pack_kernel,
        out_shape=(
            jax.ShapeDtypeStruct((half, share), BF16),
            jax.ShapeDtypeStruct((half, share), BF16),
            jax.ShapeDtypeStruct((tok, 8), F32),
        ),
        in_specs=[pl.BlockSpec(memory_space=pltpu.SMEM), vmem, vmem, vmem],
        out_specs=(vmem, vmem, vmem),
        name="pack",
    )(c, routes, weights, tokens)


def expert_kernel(first, rows, core_ref, y_ref, x_ref, xs, *refs):
    if first:
        wg, wu, wd, out, gain_out = refs[:5]
        refs = refs[5:]
        outs = [out.at[o] for o in range(4)]
    else:
        more = refs[0:3]
        wg, wu, wd, gain_in = refs[3:7]
        outs = refs[7:11]
        refs = refs[11:]
    raw, gain_s, xn, gu_s, d_s, stage, sems, osems = refs
    core = core_ref[0]
    at_outer = jnp.where(core == 0, y_ref[0], x_ref[0])

    def block(o, i):
        outer = o if first else jnp.bitwise_and(at_outer + o, 3)
        return jnp.where(core == 0, outer * 4 + i, i * 4 + outer)

    def source(o):
        if first:
            return xs.at[o]
        return xs if o == 0 else more[o - 1]

    count = [0]

    def fetch(src, dst):
        cp = pltpu.make_async_copy(src, dst, sems.at[count[0]])
        count[0] += 1
        cp.start()
        return cp

    half = rows // 2
    width = xn.shape[1]
    units = gu_s.shape[1] // 2

    def fetch_rows(at):
        return [
            fetch(source(o).at[i, pl.ds(at, half), :], raw.at[block(o, i), pl.ds(at, half), :])
            for o in range(4)
            for i in range(4)
        ]

    x_cp = [fetch_rows(0)]
    if first:
        gain_cp = [
            fetch(source(o).at[i, pl.ds(rows, GAIN_ROWS), :], gain_s.at[block(o, i)])
            for o in range(4)
            for i in range(4)
        ]
    else:
        gain_cp = [fetch(gain_in, gain_s)]
    w_cp = [fetch(wg, gu_s.at[:, pl.ds(0, units)]), fetch(wu, gu_s.at[:, pl.ds(units, units)])]
    x_cp.append(fetch_rows(half))
    d_cp = [
        fetch(
            wd.at[:, pl.ds(pl.multiple_of(block(o, i) * 128, 128), 128)],
            d_s.at[:, pl.ds((o * 4 + i) * 128, 128)],
        )
        for o in range(4)
        for i in range(4)
    ]
    for cp in gain_cp:
        cp.wait()
    copies = []

    def store(n, src, dst):
        cp = pltpu.make_async_copy(src, dst, osems.at[n])
        cp.start()
        copies.append(cp)

    if first:
        store(4, gain_s, gain_out)
    step = 32

    def norm(i):
        at = i * step
        acc = jnp.zeros((step, 128), F32)
        vals = []
        for j in range(16):
            v = raw[j, pl.ds(at, step), :].astype(F32)
            vals.append(v)
            acc = acc + v * v
        scale = lax.rsqrt(jnp.sum(acc, axis=1, keepdims=True) * (1.0 / width) + EPS)
        for j in range(16):
            gain = gain_s[j, 0:1, :].astype(F32)
            xn[pl.ds(at, step), j * 128 : (j + 1) * 128] = (vals[j] * scale * gain).astype(BF16)

    steps = half // step

    def act(gate, up):
        return (gate * up / (1.0 + jnp.exp(-gate))).astype(BF16)

    for cp in x_cp[0]:
        cp.wait()
    for i in range(steps):
        norm(i)
    w_cp[0].wait()
    gate = jnp.dot(xn[:half, :], gu_s[:, :units], preferred_element_type=F32)
    w_cp[1].wait()
    for cp in x_cp[1]:
        cp.wait()
    up = jnp.dot(xn[:half, :], gu_s[:, units:], preferred_element_type=F32)
    low = act(gate, up)
    for i in range(steps, 2 * steps):
        norm(i)
    both = jnp.dot(xn[half:, :], gu_s[...], preferred_element_type=F32)
    hidden = jnp.concatenate([low, act(both[:, :units], both[:, units:])], axis=0)
    for cp in d_cp:
        cp.wait()
    for o in range(4):
        res = jnp.dot(
            hidden, d_s[:, o * 512 : (o + 1) * 512], preferred_element_type=F32
        ).astype(BF16)
        for i in range(4):
            stage[o, i] = res[:, i * 128 : (i + 1) * 128]
        store(o, stage.at[o], outs[o])
    for cp in copies:
        cp.wait()


def expert(first, place, xs, weights, gain):
    rows = 512
    width, units = weights[0].shape
    hbm = pl.BlockSpec(memory_space=pltpu.HBM)
    if first:
        args = (*place, xs, *weights)
        outs = (
            jax.ShapeDtypeStruct((4, 4, rows, 128), BF16),
            jax.ShapeDtypeStruct((16, GAIN_ROWS, 128), BF16),
        )
    else:
        args = (*place, *xs, *weights, gain)
        outs = tuple([jax.ShapeDtypeStruct((4, rows, 128), BF16)] * 4)
    return pl.pallas_call(
        functools.partial(expert_kernel, first, rows),
        out_shape=outs,
        in_specs=[pl.BlockSpec(memory_space=pltpu.SMEM)] * 3 + [hbm] * (len(args) - 3),
        out_specs=tuple([hbm] * len(outs)),
        scratch_shapes=[
            pltpu.VMEM((16, rows, 128), BF16),
            pltpu.VMEM((16, GAIN_ROWS, 128), BF16),
            pltpu.VMEM((rows, width), BF16),
            pltpu.VMEM((width, 2 * units), BF16),
            pltpu.VMEM((units, width), BF16),
            pltpu.VMEM((4, 4, rows, 128), BF16),
            pltpu.SemaphoreType.DMA((66,)),
            pltpu.SemaphoreType.DMA((5,)),
        ],
        compiler_params=pltpu.CompilerParams(vmem_limit_bytes=63 * 1024 * 1024),
        name="expert_far" if first else "expert_near",
    )(*args)


def combine_kernel(table, rows, combined, squares):
    tok = table.shape[0]
    count = rows.shape[0]
    cols = lax.broadcasted_iota(jnp.int32, (tok, count), 1)
    total = None
    for k in range(2):
        target = table[:, k : k + 1].astype(jnp.int32)
        pick = (cols == target).astype(F32).astype(BF16)
        got = jnp.dot(pick, rows[...], preferred_element_type=F32)
        term = got * table[:, 2 + k : 3 + k]
        total = term if total is None else total + term
    combined[...] = total
    mine = jnp.sum((total * total).T, axis=0, keepdims=True)
    for i in range(squares.shape[0]):
        squares[i] = mine


def combine(table, rows):
    tok = table.shape[0]
    share = rows.shape[1]
    vmem = pl.BlockSpec(memory_space=pltpu.VMEM)
    return pl.pallas_call(
        combine_kernel,
        out_shape=(
            jax.ShapeDtypeStruct((tok, share), F32),
            jax.ShapeDtypeStruct((16, 1, tok), F32),
        ),
        in_specs=[vmem] * 2,
        out_specs=(vmem, vmem),
        name="combine",
    )(table, rows)


ALL = ("z", "c", "y", "x")


def flat(z, c, y, x):
    return ((z * 2 + c) * 4 + y) * 4 + x


def lines(along_x_for):
    groups = []
    for z in range(16):
        for c in range(2):
            for i in range(4):
                if c == along_x_for:
                    groups.append([flat(z, c, i, x) for x in range(4)])
                else:
                    groups.append([flat(z, c, y, i) for y in range(4)])
    return groups


def exchange(v, axis, groups=None):
    return lax.all_to_all(
        v, axis, split_axis=0, concat_axis=0, tiled=True, axis_index_groups=groups
    )


def across(v, along_x_for):
    return exchange(v, ALL, lines(along_x_for))


def ahead(v, along_x_for, step):
    pairs = []
    for z in range(16):
        for c in range(2):
            for y in range(4):
                for x in range(4):
                    to_y, to_x = (y, x + step) if c == along_x_for else (y + step, x)
                    pairs.append((flat(z, c, y, x), flat(z, c, to_y % 4, to_x % 4)))
    return lax.ppermute(v, ALL, pairs)


def swap(v):
    return lax.ppermute(v, "c", [(0, 1), (1, 0)])


def total_of(parts):
    total = parts[0].astype(F32)
    for p in parts[1:]:
        total = total + p.astype(F32)
    return total.astype(BF16)


def summed(v):
    return total_of([v[i] for i in range(v.shape[0])])


def copies_of(v):
    return jnp.broadcast_to(v[None], (4, *v.shape))


def over_z(near, far):
    share = near.shape[1]
    both = jnp.stack([near.reshape(16, -1, share), far.reshape(16, -1, share)], axis=1)
    return exchange(both, "z")


def local(tokens, norm_gain, w_gate, w_up, w_down, routes, route_weights, final_gain):
    _, share = tokens.shape
    width = share * 16
    place = tuple(lax.axis_index(a).astype(jnp.int32).reshape(1) for a in ("c", "y", "x"))
    near, far, table = pack(place[0], routes.T, route_weights.T, tokens)
    weights = (w_gate[0], w_up[0], w_down[0])
    both = over_z(near, swap(far))
    near, far = (both[:, i].reshape(-1, share) for i in range(2))
    gain_rows = jnp.broadcast_to(norm_gain[None, :], (GAIN_ROWS, share))
    rows = jnp.concatenate([far, gain_rows, near], axis=0)
    rows = across(copies_of(rows), 0)
    first = far.shape[0] + GAIN_ROWS
    far = across(copies_of(rows[:, :first]), 1)
    near = rows[:, first:]
    near = [near] + [ahead(near, 1, -s) for s in (1, 2, 3)]
    far, gain = expert(True, place, far, weights, None)
    far = summed(across(far, 1))
    near = expert(False, place, near, weights, gain)
    two = ahead(near[2], 1, 2)
    near = total_of([near[0], two, ahead(near[1], 1, 1), ahead(near[3], 1, 3)])
    far = swap(summed(across(far, 0)))
    near = summed(across(near, 0))
    both = over_z(near, far)
    combined, squares = combine(table, both.reshape(-1, share))
    total = exchange(squares, ("y", "x")).sum(axis=(0, 1))
    scale = lax.rsqrt(total / width + EPS)
    return (combined * scale[:, None] * final_gain.astype(F32)[None, :]).astype(BF16)


def solution(mesh):
    fine = Mesh(mesh.devices.reshape(16, 2, 4, 4), ("z", "c", "y", "x"))
    ep = ("z", "c")
    tp = ("y", "x")
    in_specs = (
        P(ep, tp),
        P(tp),
        P(ep, None, tp),
        P(ep, None, tp),
        P(ep, tp, None),
        P(ep, None),
        P(ep, None),
        P(tp),
    )
    return jax.shard_map(
        local, mesh=fine, in_specs=in_specs, out_specs=P(ep, tp), check_vma=False
    )
```

```python
import functools

import jax
import jax.numpy as jnp
from jax import lax
from jax.experimental import pallas as pl
from jax.experimental.pallas import tpu as pltpu
from jax.sharding import Mesh, PartitionSpec as P


EPS = 1e-06
F32 = jnp.float32
BF16 = jnp.bfloat16
GAIN_ROWS = 16


def pack_kernel(pos, routes, weights, tokens, gain, near, far, table, gain_out):
    tok = tokens.shape[0]
    half = near.shape[0]
    experts = 2 * lax.axis_size("z")
    cap = half // (experts // 2)
    e0 = routes[0:1, :]
    e1 = routes[1:2, :]
    lanes = lax.broadcasted_iota(jnp.int32, (experts, tok), 0)
    hot0 = lanes == e0
    hot1 = lanes == e1
    hot = (hot0 | hot1).astype(F32).astype(BF16)
    row = lax.broadcasted_iota(jnp.int32, (tok, tok), 0)
    col = lax.broadcasted_iota(jnp.int32, (tok, tok), 1)
    earlier = (row < col).astype(F32).astype(BF16)
    before = jnp.dot(hot, earlier, preferred_element_type=F32)

    def place(e, mine):
        slot = jnp.sum(jnp.where(mine, before, 0.0), axis=0, keepdims=True)
        other = jnp.bitwise_xor(jnp.bitwise_and(e, 1), pos[0])
        return other * half + (e >> 1) * cap + slot.astype(jnp.int32)

    t0 = place(e0, hot0)
    t1 = place(e1, hot1)
    for at, out in ((0, near), (half, far)):
        rows = lax.broadcasted_iota(jnp.int32, (half, tok), 0) + at
        put = ((rows == t0) | (rows == t1)).astype(F32).astype(BF16)
        out[...] = jnp.dot(put, tokens[...], preferred_element_type=F32).astype(BF16)

    def packed(t):
        other = (t >= half).astype(jnp.int32)
        inside = t - other * half
        at_z = inside // cap
        return (at_z * 2 + other) * cap + (inside - at_z * cap)

    t0 = packed(t0)
    t1 = packed(t1)
    stack = jnp.concatenate(
        [t0.astype(F32), t1.astype(F32), weights[...], jnp.zeros((4, tok), F32)], axis=0
    )
    table[...] = stack.T
    gain_out[...] = jnp.broadcast_to(gain[...], gain_out.shape)


def pack(c, routes, weights, tokens, gain):
    tok, share = tokens.shape
    half = lax.axis_size("z") * 32
    vmem = pl.BlockSpec(memory_space=pltpu.VMEM)
    return pl.pallas_call(
        pack_kernel,
        out_shape=(
            jax.ShapeDtypeStruct((half, share), BF16),
            jax.ShapeDtypeStruct((half, share), BF16),
            jax.ShapeDtypeStruct((tok, 8), F32),
            jax.ShapeDtypeStruct((GAIN_ROWS, share), BF16),
        ),
        in_specs=[pl.BlockSpec(memory_space=pltpu.SMEM)] + [vmem] * 4,
        out_specs=(vmem,) * 4,
        name="pack",
    )(c, routes, weights, tokens, gain)


def expert_kernel(first, rows, core_ref, y_ref, x_ref, xs, *refs):
    if first:
        wg, wu, wd, out, gain_out = refs[:5]
        refs = refs[5:]
        outs = [out.at[o] for o in range(4)]
    else:
        more = refs[0:3]
        wg, wu, wd, gain_in = refs[3:7]
        outs = refs[7:11]
        refs = refs[11:]
    raw, gain_s, xn, gu_s, d_s, stage, sems, osems = refs
    core = core_ref[0]
    at_outer = jnp.where(core == 0, y_ref[0], x_ref[0])

    def block(o, i):
        outer = o if first else jnp.bitwise_and(at_outer + o, 3)
        return jnp.where(core == 0, outer * 4 + i, i * 4 + outer)

    def source(o):
        if first:
            return xs.at[o]
        return xs if o == 0 else more[o - 1]

    count = [0]

    def fetch(src, dst):
        cp = pltpu.make_async_copy(src, dst, sems.at[count[0]])
        count[0] += 1
        cp.start()
        return cp

    half = rows // 2
    width = xn.shape[1]
    units = gu_s.shape[1] // 2

    def fetch_rows(at):
        return [
            fetch(source(o).at[i, pl.ds(at, half), :], raw.at[block(o, i), pl.ds(at, half), :])
            for o in range(4)
            for i in range(4)
        ]

    x_cp = [fetch_rows(0)]
    if first:
        gain_cp = [
            fetch(source(o).at[i, pl.ds(rows, GAIN_ROWS), :], gain_s.at[block(o, i)])
            for o in range(4)
            for i in range(4)
        ]
    else:
        gain_cp = [fetch(gain_in, gain_s)]
    w_cp = [fetch(wg, gu_s.at[:, pl.ds(0, units)]), fetch(wu, gu_s.at[:, pl.ds(units, units)])]
    x_cp.append(fetch_rows(half))
    d_cp = [
        fetch(
            wd.at[:, pl.ds(pl.multiple_of(block(o, i) * 128, 128), 128)],
            d_s.at[:, pl.ds((o * 4 + i) * 128, 128)],
        )
        for o in range(4)
        for i in range(4)
    ]
    for cp in gain_cp:
        cp.wait()
    copies = []

    def store(n, src, dst):
        cp = pltpu.make_async_copy(src, dst, osems.at[n])
        cp.start()
        copies.append(cp)

    if first:
        store(4, gain_s, gain_out)
    step = 32

    def norm(i):
        at = i * step
        acc = jnp.zeros((step, 128), F32)
        vals = []
        for j in range(16):
            v = raw[j, pl.ds(at, step), :].astype(F32)
            vals.append(v)
            acc = acc + v * v
        scale = lax.rsqrt(jnp.sum(acc, axis=1, keepdims=True) * (1.0 / width) + EPS)
        for j in range(16):
            gain = gain_s[j, 0:1, :].astype(F32)
            xn[pl.ds(at, step), j * 128 : (j + 1) * 128] = (vals[j] * scale * gain).astype(BF16)

    steps = half // step

    def act(gate, up):
        return (gate * up / (1.0 + jnp.exp(-gate))).astype(BF16)

    for cp in x_cp[0]:
        cp.wait()
    for i in range(steps):
        norm(i)
    w_cp[0].wait()
    gate = jnp.dot(xn[:half, :], gu_s[:, :units], preferred_element_type=F32)
    w_cp[1].wait()
    for cp in x_cp[1]:
        cp.wait()
    up = jnp.dot(xn[:half, :], gu_s[:, units:], preferred_element_type=F32)
    low = act(gate, up)
    for i in range(steps, 2 * steps):
        norm(i)
    both = jnp.dot(xn[half:, :], gu_s[...], preferred_element_type=F32)
    hidden = jnp.concatenate([low, act(both[:, :units], both[:, units:])], axis=0)
    for cp in d_cp:
        cp.wait()
    for o in range(4):
        res = jnp.dot(
            hidden, d_s[:, o * 512 : (o + 1) * 512], preferred_element_type=F32
        ).astype(BF16)
        for i in range(4):
            stage[o, i] = res[:, i * 128 : (i + 1) * 128]
        store(o, stage.at[o], outs[o])
    for cp in copies:
        cp.wait()


def expert(first, place, xs, weights, gain):
    rows = 512
    width, units = weights[0].shape
    hbm = pl.BlockSpec(memory_space=pltpu.HBM)
    if first:
        args = (*place, xs, *weights)
        outs = (
            jax.ShapeDtypeStruct((4, 4, rows, 128), BF16),
            jax.ShapeDtypeStruct((16, GAIN_ROWS, 128), BF16),
        )
    else:
        args = (*place, *xs, *weights, gain)
        outs = tuple([jax.ShapeDtypeStruct((4, rows, 128), BF16)] * 4)
    return pl.pallas_call(
        functools.partial(expert_kernel, first, rows),
        out_shape=outs,
        in_specs=[pl.BlockSpec(memory_space=pltpu.SMEM)] * 3 + [hbm] * (len(args) - 3),
        out_specs=tuple([hbm] * len(outs)),
        scratch_shapes=[
            pltpu.VMEM((16, rows, 128), BF16),
            pltpu.VMEM((16, GAIN_ROWS, 128), BF16),
            pltpu.VMEM((rows, width), BF16),
            pltpu.VMEM((width, 2 * units), BF16),
            pltpu.VMEM((units, width), BF16),
            pltpu.VMEM((4, 4, rows, 128), BF16),
            pltpu.SemaphoreType.DMA((66,)),
            pltpu.SemaphoreType.DMA((5,)),
        ],
        compiler_params=pltpu.CompilerParams(vmem_limit_bytes=63 * 1024 * 1024),
        name="expert_far" if first else "expert_near",
    )(*args)


def combine_kernel(table, rows, combined, squares):
    tok = table.shape[0]
    count = rows.shape[0]
    cols = lax.broadcasted_iota(jnp.int32, (tok, count), 1)
    picks = [(cols == table[:, k : k + 1].astype(jnp.int32)).astype(F32) for k in range(2)]
    pick = jnp.concatenate(picks, axis=0).astype(BF16)
    got = jnp.dot(pick, rows[...], preferred_element_type=F32)
    total = got[:tok] * table[:, 2:3] + got[tok:] * table[:, 3:4]
    combined[...] = total
    mine = jnp.sum((total * total).T, axis=0, keepdims=True)
    for i in range(squares.shape[0]):
        squares[i] = mine


def combine(table, rows):
    tok = table.shape[0]
    share = rows.shape[1]
    vmem = pl.BlockSpec(memory_space=pltpu.VMEM)
    return pl.pallas_call(
        combine_kernel,
        out_shape=(
            jax.ShapeDtypeStruct((tok, share), F32),
            jax.ShapeDtypeStruct((16, 1, tok), F32),
        ),
        in_specs=[vmem] * 2,
        out_specs=(vmem, vmem),
        name="combine",
    )(table, rows)


def finish_kernel(width, parts, combined, gain, out):
    total = parts[0]
    for i in range(1, parts.shape[0]):
        total = total + parts[i]
    scale = lax.rsqrt(total / width + EPS)
    column = jnp.broadcast_to(scale, (8, scale.shape[1])).T[:, 0:1]
    out[...] = (combined[...] * column * gain[...].astype(F32)).astype(BF16)


def finish(width, parts, combined, gain):
    vmem = pl.BlockSpec(memory_space=pltpu.VMEM)
    return pl.pallas_call(
        functools.partial(finish_kernel, width),
        out_shape=jax.ShapeDtypeStruct(combined.shape, BF16),
        in_specs=[vmem] * 3,
        out_specs=vmem,
        name="finish",
    )(parts, combined, gain)


ALL = ("z", "c", "y", "x")


def flat(z, c, y, x):
    return ((z * 2 + c) * 4 + y) * 4 + x


def lines(along_x_for):
    groups = []
    for z in range(16):
        for c in range(2):
            for i in range(4):
                if c == along_x_for:
                    groups.append([flat(z, c, i, x) for x in range(4)])
                else:
                    groups.append([flat(z, c, y, i) for y in range(4)])
    return groups


def exchange(v, axis, groups=None):
    return lax.all_to_all(
        v, axis, split_axis=0, concat_axis=0, tiled=True, axis_index_groups=groups
    )


def across(v, along_x_for):
    return exchange(v, ALL, lines(along_x_for))


def ahead(v, along_x_for, step):
    pairs = []
    for z in range(16):
        for c in range(2):
            for y in range(4):
                for x in range(4):
                    to_y, to_x = (y, x + step) if c == along_x_for else (y + step, x)
                    pairs.append((flat(z, c, y, x), flat(z, c, to_y % 4, to_x % 4)))
    return lax.ppermute(v, ALL, pairs)


def swap(v):
    return lax.ppermute(v, "c", [(0, 1), (1, 0)])


def total_of(parts):
    total = parts[0].astype(F32)
    for p in parts[1:]:
        total = total + p.astype(F32)
    return total.astype(BF16)


def summed(v):
    return total_of([v[i] for i in range(v.shape[0])])


def copies_of(v):
    return jnp.broadcast_to(v[None], (4, *v.shape))


def over_z(near, far):
    share = near.shape[1]
    both = jnp.stack([near.reshape(16, -1, share), far.reshape(16, -1, share)], axis=1)
    return exchange(both, "z")


def local(tokens, norm_gain, w_gate, w_up, w_down, routes, route_weights, final_gain):
    _, share = tokens.shape
    width = share * 16
    place = tuple(lax.axis_index(a).astype(jnp.int32).reshape(1) for a in ("c", "y", "x"))
    near, far, table, gain_rows = pack(
        place[0], routes.T, route_weights.T, tokens, norm_gain[None, :]
    )
    weights = (w_gate[0], w_up[0], w_down[0])
    both = over_z(near, swap(far))
    near, far = (both[:, i].reshape(-1, share) for i in range(2))
    rows = jnp.concatenate([far, gain_rows, near], axis=0)
    rows = across(copies_of(rows), 0)
    first = far.shape[0] + GAIN_ROWS
    far = across(copies_of(rows[:, :first]), 1)
    near = rows[:, first:]
    near = [near] + [ahead(near, 1, -s) for s in (1, 2, 3)]
    far, gain = expert(True, place, far, weights, None)
    far = summed(across(far, 1))
    near = expert(False, place, near, weights, gain)
    two = ahead(near[2], 1, 2)
    near = total_of([near[0], two, ahead(near[1], 1, 1), ahead(near[3], 1, 3)])
    far = swap(summed(across(far, 0)))
    near = summed(across(near, 0))
    both = over_z(near, far)
    combined, squares = combine(table, both.reshape(-1, share))
    parts = exchange(squares, ("y", "x"))
    return finish(width, parts, combined, final_gain[None, :])


def solution(mesh):
    fine = Mesh(mesh.devices.reshape(16, 2, 4, 4), ("z", "c", "y", "x"))
    ep = ("z", "c")
    tp = ("y", "x")
    in_specs = (
        P(ep, tp),
        P(tp),
        P(ep, None, tp),
        P(ep, None, tp),
        P(ep, tp, None),
        P(ep, None),
        P(ep, None),
        P(tp),
    )
    return jax.shard_map(
        local, mesh=fine, in_specs=in_specs, out_specs=P(ep, tp), check_vma=False
    )
```

```python
import functools

import jax
import jax.numpy as jnp
from jax import lax
from jax.experimental import pallas as pl
from jax.experimental.pallas import tpu as pltpu
from jax.sharding import Mesh, PartitionSpec as P


EPS = 1e-06
F32 = jnp.float32
BF16 = jnp.bfloat16
GAIN_ROWS = 16


def pack_kernel(pos, routes, weights, tokens, out, table):
    tok = tokens.shape[0]
    count = out.shape[0]
    experts = 2 * lax.axis_size("z")
    cap = count // experts
    e0 = routes[0:1, :]
    e1 = routes[1:2, :]
    names = lax.broadcasted_iota(jnp.int32, (experts, tok), 0)
    hot0 = names == e0
    hot1 = names == e1
    hot = (hot0 | hot1).astype(F32).astype(BF16)
    row = lax.broadcasted_iota(jnp.int32, (tok, tok), 0)
    col = lax.broadcasted_iota(jnp.int32, (tok, tok), 1)
    earlier = (row < col).astype(F32).astype(BF16)
    before = jnp.dot(hot, earlier, preferred_element_type=F32)

    def place(e, mine):
        slot = jnp.sum(jnp.where(mine, before, 0.0), axis=0, keepdims=True)
        return jnp.bitwise_xor(e, pos[0]) * cap + slot.astype(jnp.int32)

    t0 = place(e0, hot0)
    t1 = place(e1, hot1)
    rows = lax.broadcasted_iota(jnp.int32, (count, tok), 0)
    put = ((rows == t0) | (rows == t1)).astype(F32).astype(BF16)
    out[...] = jnp.dot(put, tokens[...], preferred_element_type=F32).astype(BF16)
    stack = jnp.concatenate(
        [t0.astype(F32), t1.astype(F32), weights[...], jnp.zeros((4, tok), F32)], axis=0
    )
    table[...] = stack.T


def pack(c, routes, weights, tokens):
    tok, share = tokens.shape
    count = 2 * lax.axis_size("z") * 32
    vmem = pl.BlockSpec(memory_space=pltpu.VMEM)
    return pl.pallas_call(
        pack_kernel,
        out_shape=(
            jax.ShapeDtypeStruct((count, share), BF16),
            jax.ShapeDtypeStruct((tok, 8), F32),
        ),
        in_specs=[pl.BlockSpec(memory_space=pltpu.SMEM), vmem, vmem, vmem],
        out_specs=(vmem, vmem),
        name="pack",
    )(c, routes, weights, tokens)


def expert_kernel(first, rows, core_ref, y_ref, x_ref, xs, *refs):
    if first:
        wg, wu, wd, out, gain_out = refs[:5]
        refs = refs[5:]
        outs = [out.at[o] for o in range(4)]
    else:
        more = refs[0:3]
        wg, wu, wd, gain_in = refs[3:7]
        outs = refs[7:11]
        refs = refs[11:]
    raw, gain_s, xn, gu_s, d_s, stage, sems, osems = refs
    core = core_ref[0]
    at_outer = jnp.where(core == 0, y_ref[0], x_ref[0])

    def block(o, i):
        outer = o if first else jnp.bitwise_and(at_outer + o, 3)
        return jnp.where(core == 0, outer * 4 + i, i * 4 + outer)

    def source(o):
        if first:
            return xs.at[o]
        return xs if o == 0 else more[o - 1]

    count = [0]

    def fetch(src, dst):
        cp = pltpu.make_async_copy(src, dst, sems.at[count[0]])
        count[0] += 1
        cp.start()
        return cp

    half = rows // 2
    width = xn.shape[1]
    units = gu_s.shape[1] // 2

    def fetch_rows(at):
        return [
            fetch(source(o).at[i, pl.ds(at, half), :], raw.at[block(o, i), pl.ds(at, half), :])
            for o in range(4)
            for i in range(4)
        ]

    x_cp = [fetch_rows(0)]
    if first:
        gain_cp = [
            fetch(source(o).at[i, pl.ds(rows, GAIN_ROWS), :], gain_s.at[block(o, i)])
            for o in range(4)
            for i in range(4)
        ]
    else:
        gain_cp = [fetch(gain_in, gain_s)]
    w_cp = [fetch(wg, gu_s.at[:, pl.ds(0, units)]), fetch(wu, gu_s.at[:, pl.ds(units, units)])]
    x_cp.append(fetch_rows(half))
    d_cp = [
        fetch(
            wd.at[:, pl.ds(pl.multiple_of(block(o, i) * 128, 128), 128)],
            d_s.at[:, pl.ds((o * 4 + i) * 128, 128)],
        )
        for o in range(4)
        for i in range(4)
    ]
    for cp in gain_cp:
        cp.wait()
    copies = []

    def store(n, src, dst):
        cp = pltpu.make_async_copy(src, dst, osems.at[n])
        cp.start()
        copies.append(cp)

    if first:
        store(4, gain_s, gain_out)
    step = 32

    def norm(i):
        at = i * step
        acc = jnp.zeros((step, 128), F32)
        vals = []
        for j in range(16):
            v = raw[j, pl.ds(at, step), :].astype(F32)
            vals.append(v)
            acc = acc + v * v
        scale = lax.rsqrt(jnp.sum(acc, axis=1, keepdims=True) * (1.0 / width) + EPS)
        for j in range(16):
            gain = gain_s[j, 0:1, :].astype(F32)
            xn[pl.ds(at, step), j * 128 : (j + 1) * 128] = (vals[j] * scale * gain).astype(BF16)

    steps = half // step

    def act(gate, up):
        return (gate * up / (1.0 + jnp.exp(-gate))).astype(BF16)

    for cp in x_cp[0]:
        cp.wait()
    for i in range(steps):
        norm(i)
    w_cp[0].wait()
    gate = jnp.dot(xn[:half, :], gu_s[:, :units], preferred_element_type=F32)
    w_cp[1].wait()
    for cp in x_cp[1]:
        cp.wait()
    up = jnp.dot(xn[:half, :], gu_s[:, units:], preferred_element_type=F32)
    low = act(gate, up)
    for i in range(steps, 2 * steps):
        norm(i)
    both = jnp.dot(xn[half:, :], gu_s[...], preferred_element_type=F32)
    hidden = jnp.concatenate([low, act(both[:, :units], both[:, units:])], axis=0)
    for cp in d_cp:
        cp.wait()
    for o in range(4):
        res = jnp.dot(
            hidden, d_s[:, o * 512 : (o + 1) * 512], preferred_element_type=F32
        ).astype(BF16)
        for i in range(4):
            stage[o, i] = res[:, i * 128 : (i + 1) * 128]
        store(o, stage.at[o], outs[o])
    for cp in copies:
        cp.wait()


def expert(first, place, xs, weights, gain):
    rows = 512
    width, units = weights[0].shape
    hbm = pl.BlockSpec(memory_space=pltpu.HBM)
    if first:
        args = (*place, xs, *weights)
        outs = (
            jax.ShapeDtypeStruct((4, 4, rows, 128), BF16),
            jax.ShapeDtypeStruct((16, GAIN_ROWS, 128), BF16),
        )
    else:
        args = (*place, *xs, *weights, gain)
        outs = tuple([jax.ShapeDtypeStruct((4, rows, 128), BF16)] * 4)
    return pl.pallas_call(
        functools.partial(expert_kernel, first, rows),
        out_shape=outs,
        in_specs=[pl.BlockSpec(memory_space=pltpu.SMEM)] * 3 + [hbm] * (len(args) - 3),
        out_specs=tuple([hbm] * len(outs)),
        scratch_shapes=[
            pltpu.VMEM((16, rows, 128), BF16),
            pltpu.VMEM((16, GAIN_ROWS, 128), BF16),
            pltpu.VMEM((rows, width), BF16),
            pltpu.VMEM((width, 2 * units), BF16),
            pltpu.VMEM((units, width), BF16),
            pltpu.VMEM((4, 4, rows, 128), BF16),
            pltpu.SemaphoreType.DMA((66,)),
            pltpu.SemaphoreType.DMA((5,)),
        ],
        compiler_params=pltpu.CompilerParams(vmem_limit_bytes=63 * 1024 * 1024),
        name="expert_far" if first else "expert_near",
    )(*args)


def combine_kernel(table, rows, combined, squares):
    tok = table.shape[0]
    count = rows.shape[0]
    cols = lax.broadcasted_iota(jnp.int32, (tok, count), 1)
    total = None
    for k in range(2):
        target = table[:, k : k + 1].astype(jnp.int32)
        pick = (cols == target).astype(F32).astype(BF16)
        got = jnp.dot(pick, rows[...], preferred_element_type=F32)
        term = got * table[:, 2 + k : 3 + k]
        total = term if total is None else total + term
    combined[...] = total
    mine = jnp.sum((total * total).T, axis=0, keepdims=True)
    for i in range(squares.shape[0]):
        squares[i] = mine


def combine(table, rows):
    tok = table.shape[0]
    share = rows.shape[1]
    vmem = pl.BlockSpec(memory_space=pltpu.VMEM)
    return pl.pallas_call(
        combine_kernel,
        out_shape=(
            jax.ShapeDtypeStruct((tok, share), F32),
            jax.ShapeDtypeStruct((16, 1, tok), F32),
        ),
        in_specs=[vmem] * 2,
        out_specs=(vmem, vmem),
        name="combine",
    )(table, rows)


ALL = ("z", "c", "y", "x")


def flat(z, c, y, x):
    return ((z * 2 + c) * 4 + y) * 4 + x


def lines(along_x_for):
    groups = []
    for z in range(16):
        for c in range(2):
            for i in range(4):
                if c == along_x_for:
                    groups.append([flat(z, c, i, x) for x in range(4)])
                else:
                    groups.append([flat(z, c, y, i) for y in range(4)])
    return groups


def exchange(v, axis, groups=None):
    return lax.all_to_all(
        v, axis, split_axis=0, concat_axis=0, tiled=True, axis_index_groups=groups
    )


def across(v, along_x_for):
    return exchange(v, ALL, lines(along_x_for))


def ahead(v, along_x_for, step):
    pairs = []
    for z in range(16):
        for c in range(2):
            for y in range(4):
                for x in range(4):
                    to_y, to_x = (y, x + step) if c == along_x_for else (y + step, x)
                    pairs.append((flat(z, c, y, x), flat(z, c, to_y % 4, to_x % 4)))
    return lax.ppermute(v, ALL, pairs)


def swap(v):
    return lax.ppermute(v, "c", [(0, 1), (1, 0)])


def total_of(parts):
    total = parts[0].astype(F32)
    for p in parts[1:]:
        total = total + p.astype(F32)
    return total.astype(BF16)


def summed(v):
    return total_of([v[i] for i in range(v.shape[0])])


def copies_of(v):
    return jnp.broadcast_to(v[None], (4, *v.shape))


def over_z(near, far):
    share = near.shape[1]
    both = jnp.stack([near.reshape(16, -1, share), far.reshape(16, -1, share)], axis=1)
    return exchange(both, "z")


def local(tokens, norm_gain, w_gate, w_up, w_down, routes, route_weights, final_gain):
    _, share = tokens.shape
    width = share * 16
    place = tuple(lax.axis_index(a).astype(jnp.int32).reshape(1) for a in ("c", "y", "x"))
    rows, table = pack(place[0], routes.T, route_weights.T, tokens)
    weights = (w_gate[0], w_up[0], w_down[0])
    both = exchange(rows.reshape(16, 2, -1, share), "z")
    near, far = (both[:, i].reshape(-1, share) for i in range(2))
    far = swap(far)
    gain_rows = jnp.broadcast_to(norm_gain[None, :], (GAIN_ROWS, share))
    rows = jnp.concatenate([far, gain_rows, near], axis=0)
    rows = across(copies_of(rows), 0)
    first = far.shape[0] + GAIN_ROWS
    far = across(copies_of(rows[:, :first]), 1)
    near = rows[:, first:]
    near = [near] + [ahead(near, 1, -s) for s in (1, 2, 3)]
    far, gain = expert(True, place, far, weights, None)
    far = summed(across(far, 1))
    near = expert(False, place, near, weights, gain)
    two = ahead(near[2], 1, 2)
    near = total_of([near[0], two, ahead(near[1], 1, 1), ahead(near[3], 1, 3)])
    far = swap(summed(across(far, 0)))
    near = summed(across(near, 0))
    both = over_z(near, far)
    combined, squares = combine(table, both.reshape(-1, share))
    total = exchange(squares, ("y", "x")).sum(axis=(0, 1))
    scale = lax.rsqrt(total / width + EPS)
    return (combined * scale[:, None] * final_gain.astype(F32)[None, :]).astype(BF16)


def solution(mesh):
    fine = Mesh(mesh.devices.reshape(16, 2, 4, 4), ("z", "c", "y", "x"))
    ep = ("z", "c")
    tp = ("y", "x")
    in_specs = (
        P(ep, tp),
        P(tp),
        P(ep, None, tp),
        P(ep, None, tp),
        P(ep, tp, None),
        P(ep, None),
        P(ep, None),
        P(tp),
    )
    return jax.shard_map(
        local, mesh=fine, in_specs=in_specs, out_specs=P(ep, tp), check_vma=False
    )
```
